256 devices in a mesh: row: 32 (over z, x), col: 8 (over y, core).
Axes of the slice: x: 4, y: 4, z: 8, core: 2. Of those that a mesh axis runs over, the one named last changes fastest.
Arguments:
- tokens: bfloat16 [2, 32768, 2048], P(None, ('row', 'col')), may hold values from -6 to 6
- norm_gain: float32 [2048], replicated, may hold values from 0.1 to 1.9
- mix_weight: bfloat16 [2048, 1024], replicated, may hold values from -0.125 to 0.125
- gate_weight: bfloat16 [2048, 2048], replicated, may hold values from -0.125 to 0.125
- out_weight: bfloat16 [1024, 2048], replicated, may hold values from -0.1875 to 0.1875
Outputs:
- gated: bfloat16 [2, 32768, 2048], P(None, ('row', 'col'))
The draws below stay inside these ranges and needn't reach their ends.
All inputs are finite; a program needn't handle non-finite values.
Results may differ from the reference program's by a relative error of at most 0.017.
Values may be sent and summed in bfloat16 or wider, within the bound.
No kernel may reach another device: no remote copies, remote signals or barrier semaphores. Data moves between devices by JAX's collectives and lax.ppermute only.
A program may use at most 128 MiB of HBM per device.

```python
import jax
import jax.numpy as jnp
from jax import lax

D = 2048
GROUPS = 8
GROUP_DIM = 128
FW = 1024
LENGTH = 32768
SEQS = 2


def steps_of(key, dims, split, low, high):
    gain, own = 1.0, jax.random.fold_in(key, 6)
    for dim, shards_of in split:
        steps = jnp.exp(jax.random.uniform(jax.random.fold_in(own, dim), (shards_of,), jnp.float32, low / len(split), high / len(split)))
        gain = gain * jnp.repeat(steps, dims[dim] // shards_of).reshape([-1 if axis == dim else 1 for axis in range(len(dims))])
    return gain


def bell_draw(key, dims, spread, reach, split=(), dtype=jnp.bfloat16):
    loudness = steps_of(key, dims, split, -0.22, 0.18) if split else 1.0
    entries = jax.random.normal(key, dims, jnp.float32) * spread * loudness
    return jnp.minimum(jnp.maximum(entries, -reach), reach).astype(dtype)


def setup_inputs(seed: int = 0) -> dict:
    streams_of = jax.random.split(jax.random.key(seed), 6)
    tokens = bell_draw(streams_of[0], (SEQS, LENGTH, D), 1.0, 6.0, ((1, 256),))
    norm_gain = jnp.clip(1.0 + 0.18 * jax.random.normal(streams_of[1], (D,), jnp.float32), 0.1, 1.9)
    mix_weight = bell_draw(streams_of[2], (D, FW), D ** -0.5, 0.125)
    gate_weight = bell_draw(streams_of[3], (D, D), D ** -0.5, 0.125)
    out_weight = bell_draw(streams_of[4], (FW, D), FW ** -0.5, 0.1875)
    return {"tokens": tokens, "norm_gain": norm_gain, "mix_weight": mix_weight, "gate_weight": gate_weight, "out_weight": out_weight}


def reference(tokens, norm_gain, mix_weight, gate_weight, out_weight):

    def one_sequence(sequence):
        widened = sequence.astype(jnp.float32)
        inverse_rms = lax.rsqrt(lax.optimization_barrier(jnp.mean(widened * widened, axis=-1, keepdims=True)) + 1e-06)
        normed = (widened * inverse_rms * norm_gain.astype(jnp.float32)).astype(jnp.bfloat16)
        mixed_in = jnp.dot(normed, mix_weight, preferred_element_type=jnp.float32).astype(jnp.bfloat16)
        gate_value = jax.nn.sigmoid(jnp.dot(normed, gate_weight, preferred_element_type=jnp.float32))
        grouped = mixed_in.astype(jnp.float32).reshape(LENGTH, GROUPS, GROUP_DIM)
        spectrum = jnp.fft.fft2(grouped, axes=(0, 2), norm='ortho').real
        spectral = spectrum.reshape(LENGTH, GROUPS * GROUP_DIM).astype(jnp.bfloat16)
        mapped = jnp.dot(spectral, out_weight, preferred_element_type=jnp.float32)
        return (gate_value * mapped).astype(jnp.bfloat16)
    return lax.map(one_sequence, tokens)
```

```python
import jax
import jax.numpy as jnp
import numpy as np
from jax import lax
from jax.experimental import pallas as pl
from jax.experimental.pallas import tpu as pltpu
from jax.sharding import PartitionSpec as P

AXES = ("row", "col")
DEVICES = 256
SEQS = 2
BLOCK = 128
D = 2048
GROUPS = 8
GROUP_DIM = 128
FW = GROUPS * GROUP_DIM
LENGTH = 32768
PAIRS = 4
ROWS = 2 * PAIRS
NT = (((1,), (1,)), ((), ()))
F32, BF16 = jnp.float32, jnp.bfloat16


def group_table():
    table = np.zeros((GROUP_DIM, GROUP_DIM))
    j = np.arange(GROUP_DIM)
    for i in range(GROUP_DIM // ROWS):
        for p in range(PAIRS):
            k = PAIRS * i + p
            table[i * ROWS + p] = np.cos(2 * np.pi * j * k / GROUP_DIM)
            table[i * ROWS + PAIRS + p] = np.sin(2 * np.pi * j * k / GROUP_DIM)
    table[PAIRS] = np.cos(np.pi * j)
    return table / 8


def channel_order():
    order = np.zeros((GROUP_DIM, GROUP_DIM))
    for i in range(GROUP_DIM // ROWS):
        for p in range(PAIRS):
            k = PAIRS * i + p
            order[i * ROWS + p, k] = 1
            order[i * ROWS + PAIRS + p, (GROUP_DIM - k) if k else GROUP_DIM // 2] = 1
    return order


def first_table():
    m, d = np.arange(DEVICES)[:, None], np.arange(DEVICES)[None, :]
    angle = 2 * np.pi * (m * d % DEVICES) / DEVICES
    return np.concatenate([np.cos(angle), np.sin(angle)], axis=0) / 16


def twiddle():
    m, l = np.arange(DEVICES)[:, None], np.arange(BLOCK)[None, :]
    angle = 2 * np.pi * (m * l) / LENGTH
    return np.stack([np.cos(angle), np.sin(angle)])


def second_table():
    m, l = np.arange(BLOCK)[:, None], np.arange(BLOCK)[None, :]
    angle = 2 * np.pi * (m * l % BLOCK) / BLOCK
    return np.concatenate([np.cos(angle), -np.sin(angle)], axis=1) / 16


def enter_body(tokens, gain, weight, table, out, normed):
    @pl.when(pl.program_id(0) == 0)
    def _():
        for s in range(SEQS):

            def rows(i, _):
                at = pl.ds(pl.multiple_of(i * 16, 16), 16)
                t = tokens[s, at, :].astype(F32)
                inv = lax.rsqrt(jnp.mean(t * t, axis=-1, keepdims=True) + 1e-6)
                to = pl.ds(pl.multiple_of(s * BLOCK + i * 16, 16), 16)
                normed[to, :] = (t * inv * gain[...]).astype(BF16)
                return 0

            lax.fori_loop(0, BLOCK // 16, rows, 0)

    mixed = jnp.dot(normed[...], weight[...], preferred_element_type=F32).astype(BF16)
    for q in range(mixed.shape[1] // GROUP_DIM):
        at = slice(q * GROUP_DIM, (q + 1) * GROUP_DIM)
        turned = lax.dot_general(table[...], mixed[:, at], NT, preferred_element_type=F32)
        for s in range(SEQS):
            out[s, at, :] = turned[:, s * BLOCK : (s + 1) * BLOCK].astype(BF16)


def enter(tokens, gain, weight):
    steps = 4
    wide = FW // steps
    return pl.pallas_call(
        enter_body,
        grid=(steps,),
        in_specs=[
            pl.BlockSpec((SEQS, BLOCK, D), lambda j: (0, 0, 0)),
            pl.BlockSpec((1, D), lambda j: (0, 0)),
            pl.BlockSpec((D, wide), lambda j: (0, j)),
            pl.BlockSpec((GROUP_DIM, GROUP_DIM), lambda j: (0, 0)),
        ],
        out_specs=[
            pl.BlockSpec((SEQS, wide, BLOCK), lambda j: (0, j, 0)),
            pl.BlockSpec((SEQS * BLOCK, D), lambda j: (0, 0)),
        ],
        out_shape=[
            jax.ShapeDtypeStruct((SEQS, FW, BLOCK), BF16),
            jax.ShapeDtypeStruct((SEQS * BLOCK, D), BF16),
        ],
        name="enter",
    )(tokens, gain.reshape(1, D), weight, jnp.asarray(group_table(), BF16))


def length_body(lone, x, first, twist, second, y, wide_in, wide_out):
    wide_in[...] = x[...].astype(F32)
    own = lone[0]
    cos, sin = twist[0], twist[1]
    for p in range(PAIRS):
        pair = jnp.concatenate(
            [
                wide_in[pl.ds(p, DEVICES, stride=ROWS), :].astype(BF16),
                wide_in[pl.ds(PAIRS + p, DEVICES, stride=ROWS), :].astype(BF16),
            ],
            axis=1,
        )
        both = jnp.dot(first[...], pair, preferred_element_type=F32)
        parts = []
        for q in range(2):
            real = both[:DEVICES, q * BLOCK : (q + 1) * BLOCK]
            imag = both[DEVICES:, q * BLOCK : (q + 1) * BLOCK]
            if q == 0:
                c, s = cos, sin
            elif p == 0:
                c, s = own * cos + (1 - own) * sin, own * sin - (1 - own) * cos
            else:
                c, s = sin, -cos
            turned = jnp.concatenate(
                [(real * c - imag * s).astype(BF16), (real * s + imag * c).astype(BF16)], axis=1
            )
            parts.append(lax.dot_general(second[...], turned, NT, preferred_element_type=F32))
        if p == 0:
            low, high = parts[0] - (1 - own) * parts[1], (1 - own) * parts[0] + parts[1]
        else:
            low, high = parts[0] - parts[1], parts[0] + parts[1]
        for h in range(2):
            at = slice(h * BLOCK, (h + 1) * BLOCK)
            wide_out[pl.ds(h * ROWS + p, BLOCK, stride=2 * ROWS), :] = low[:, at]
            wide_out[pl.ds(h * ROWS + PAIRS + p, BLOCK, stride=2 * ROWS), :] = high[:, at]
    y[...] = wide_out[...].astype(BF16)


def length_transform(x, lone):
    vmem = pl.BlockSpec(memory_space=pltpu.VMEM)
    rows = DEVICES * ROWS
    return pl.pallas_call(
        length_body,
        in_specs=[pl.BlockSpec(memory_space=pltpu.SMEM), vmem, vmem, vmem, vmem],
        out_specs=vmem,
        out_shape=jax.ShapeDtypeStruct((rows, BLOCK), BF16),
        scratch_shapes=[pltpu.VMEM((rows, BLOCK), F32), pltpu.VMEM((rows, BLOCK), F32)],
        name="length",
    )(
        lone,
        x,
        jnp.asarray(first_table(), BF16),
        jnp.asarray(twiddle(), F32),
        jnp.asarray(second_table(), BF16),
    )


def gate_body(normed, weight, out):
    logits = jnp.dot(normed[...], weight[...], preferred_element_type=F32)
    out[...] = jax.nn.sigmoid(logits)


def gate(normed, weight):
    steps = 8
    wide = D // steps
    return pl.pallas_call(
        gate_body,
        grid=(steps,),
        in_specs=[
            pl.BlockSpec((SEQS * BLOCK, D), lambda j: (0, 0)),
            pl.BlockSpec((D, wide), lambda j: (0, j)),
        ],
        out_specs=pl.BlockSpec((SEQS * BLOCK, wide), lambda j: (0, j)),
        out_shape=jax.ShapeDtypeStruct((SEQS * BLOCK, D), F32),
        cost_estimate=pl.CostEstimate(
            flops=2 * SEQS * BLOCK * D * D, transcendentals=SEQS * BLOCK * D, bytes_accessed=2 * D * D
        ),
        name="gate",
    )(normed, weight)


def leave_body(z, order, eye, weight, gates, out, spectral):
    @pl.when(pl.program_id(0) == 0)
    def _():
        for s in range(SEQS):
            for g in range(GROUPS):
                rows = z[pl.ds(s * FW + g * GROUP_DIM, GROUP_DIM), :]
                turned = lax.dot_general(eye[...], rows, NT, preferred_element_type=F32)
                placed = jnp.dot(turned.astype(BF16), order[...], preferred_element_type=F32)
                spectral[s * BLOCK : (s + 1) * BLOCK, g * GROUP_DIM : (g + 1) * GROUP_DIM] = (
                    placed.astype(BF16)
                )

    mapped = jnp.dot(spectral[...], weight[...], preferred_element_type=F32)
    gated = (gates[...] * mapped).astype(BF16)
    for s in range(SEQS):
        out[s] = gated[s * BLOCK : (s + 1) * BLOCK]


def leave(z, gates, weight):
    steps = 4
    wide = D // steps
    square = pl.BlockSpec((GROUP_DIM, GROUP_DIM), lambda j: (0, 0))
    return pl.pallas_call(
        leave_body,
        grid=(steps,),
        in_specs=[
            pl.BlockSpec((SEQS * FW, BLOCK), lambda j: (0, 0)),
            square,
            square,
            pl.BlockSpec((FW, wide), lambda j: (0, j)),
            pl.BlockSpec((SEQS * BLOCK, wide), lambda j: (0, j)),
        ],
        out_specs=pl.BlockSpec((SEQS, BLOCK, wide), lambda j: (0, 0, j)),
        out_shape=jax.ShapeDtypeStruct((SEQS, BLOCK, D), BF16),
        scratch_shapes=[pltpu.VMEM((SEQS * BLOCK, FW), BF16)],
        name="leave",
    )(z, jnp.asarray(channel_order(), BF16), jnp.asarray(np.eye(GROUP_DIM), BF16), weight, gates)


def exchange(x):
    return lax.all_to_all(x.reshape(DEVICES, ROWS, BLOCK), AXES, 0, 0, tiled=True).reshape(
        DEVICES * ROWS, BLOCK
    )


def local(tokens, norm_gain, mix_weight, gate_weight, out_weight):
    spectra, normed = enter(tokens, norm_gain, mix_weight)
    lone = (lax.axis_index(AXES) % (GROUP_DIM // ROWS) == 0).astype(F32).reshape(1)
    arrived = exchange(spectra)
    gates = gate(normed, gate_weight)
    returned = exchange(length_transform(arrived, lone))
    return leave(returned, gates, out_weight)


def solution(mesh):
    return jax.shard_map(
        local,
        mesh=mesh,
        in_specs=(P(None, AXES, None), P(), P(), P(), P()),
        out_specs=P(None, AXES, None),
        check_vma=False,
    )
```

```python
import jax
import jax.numpy as jnp
import numpy as np
from jax import lax
from jax.experimental import pallas as pl
from jax.experimental.pallas import tpu as pltpu
from jax.sharding import PartitionSpec as P

AXES = ("row", "col")
DEVICES = 256
SEQS = 2
BLOCK = 128
D = 2048
GROUPS = 8
GROUP_DIM = 128
FW = GROUPS * GROUP_DIM
LENGTH = 32768
PAIRS = 4
ROWS = 2 * PAIRS
NT = (((1,), (1,)), ((), ()))
F32, BF16 = jnp.float32, jnp.bfloat16
LEAVE = 4
SMALL = pltpu.CompilerParams(vmem_limit_bytes=16 * 2**20)


def in_hbm(x):
    return pltpu.with_memory_space_constraint(x, pltpu.HBM)


def in_vmem(x):
    return pltpu.with_memory_space_constraint(x, pltpu.VMEM)


def group_table():
    table = np.zeros((GROUP_DIM, GROUP_DIM))
    j = np.arange(GROUP_DIM)
    for i in range(GROUP_DIM // ROWS):
        for p in range(PAIRS):
            k = PAIRS * i + p
            table[i * ROWS + p] = np.cos(2 * np.pi * j * k / GROUP_DIM)
            table[i * ROWS + PAIRS + p] = np.sin(2 * np.pi * j * k / GROUP_DIM)
    table[PAIRS] = np.cos(np.pi * j)
    return table / 8


def channel_order():
    order = np.zeros((GROUP_DIM, GROUP_DIM))
    for i in range(GROUP_DIM // ROWS):
        for p in range(PAIRS):
            k = PAIRS * i + p
            order[i * ROWS + p, k] = 1
            order[i * ROWS + PAIRS + p, (GROUP_DIM - k) if k else GROUP_DIM // 2] = 1
    return order


def first_table():
    m, d = np.arange(DEVICES)[:, None], np.arange(DEVICES)[None, :]
    angle = 2 * np.pi * (m * d % DEVICES) / DEVICES
    return np.concatenate([np.cos(angle), np.sin(angle)], axis=0) / 16


def twiddle():
    m, l = np.arange(DEVICES)[:, None], np.arange(BLOCK)[None, :]
    angle = 2 * np.pi * (m * l) / LENGTH
    return np.stack([np.cos(angle), np.sin(angle)])


def second_table():
    m, l = np.arange(BLOCK)[:, None], np.arange(BLOCK)[None, :]
    angle = 2 * np.pi * (m * l % BLOCK) / BLOCK
    return np.concatenate([np.cos(angle), -np.sin(angle)], axis=1) / 16


def enter_body(tokens, gain, weight, table, out, saved, held, normed, matrix, sems):
    copies = [pltpu.make_async_copy(tokens.at[s], held.at[s], sems.at[s]) for s in range(SEQS)]
    copies.append(pltpu.make_async_copy(weight, matrix, sems.at[SEQS]))
    for copy in copies:
        copy.start()
    for s in range(SEQS):
        copies[s].wait()

        def rows(i, _):
            at = pl.ds(pl.multiple_of(i * 16, 16), 16)
            t = held[s, at, :].astype(F32)
            inv = lax.rsqrt(jnp.mean(t * t, axis=-1, keepdims=True) + 1e-6)
            to = pl.ds(pl.multiple_of(s * BLOCK + i * 16, 16), 16)
            normed[to, :] = (t * inv * gain[...]).astype(BF16)
            return 0

        lax.fori_loop(0, BLOCK // 16, rows, 0, unroll=4)
    save = pltpu.make_async_copy(normed, saved, sems.at[SEQS + 1])
    save.start()
    copies[SEQS].wait()
    for c in range(FW // 256):
        mixed = jnp.dot(
            normed[...], matrix[:, c * 256 : (c + 1) * 256], preferred_element_type=F32
        ).astype(BF16)
        for q in range(2):
            turned = lax.dot_general(
                table[...],
                mixed[:, q * GROUP_DIM : (q + 1) * GROUP_DIM],
                NT,
                preferred_element_type=F32,
            )
            at = slice(c * 256 + q * GROUP_DIM, c * 256 + (q + 1) * GROUP_DIM)
            for s in range(SEQS):
                out[s, at, :] = turned[:, s * BLOCK : (s + 1) * BLOCK].astype(BF16)
    save.wait()


def enter(tokens, gain, weight):
    vmem = pl.BlockSpec(memory_space=pltpu.VMEM)
    hbm = pl.BlockSpec(memory_space=pltpu.HBM)
    return pl.pallas_call(
        enter_body,
        in_specs=[hbm, vmem, hbm, vmem],
        out_specs=[vmem, hbm],
        out_shape=[
            jax.ShapeDtypeStruct((SEQS, FW, BLOCK), BF16),
            pltpu.HBM((SEQS * BLOCK, D), BF16),
        ],
        scratch_shapes=[
            pltpu.VMEM((SEQS, BLOCK, D), BF16),
            pltpu.VMEM((SEQS * BLOCK, D), BF16),
            pltpu.VMEM((D, FW), BF16),
            pltpu.SemaphoreType.DMA((SEQS + 2,)),
        ],
        compiler_params=SMALL,
        name="enter",
    )(in_hbm(tokens), gain.reshape(1, D), in_hbm(weight), jnp.asarray(group_table(), BF16))


def length_body(lone, x, first, twist, second, y, wide_in, wide_out):
    wide_in[...] = x[...].astype(F32)
    own = lone[0]
    cos, sin = twist[0], twist[1]
    for p in range(PAIRS):
        pair = jnp.concatenate(
            [
                wide_in[pl.ds(p, DEVICES, stride=ROWS), :].astype(BF16),
                wide_in[pl.ds(PAIRS + p, DEVICES, stride=ROWS), :].astype(BF16),
            ],
            axis=1,
        )
        both = jnp.dot(first[...], pair, preferred_element_type=F32)
        parts = []
        for q in range(2):
            real = both[:DEVICES, q * BLOCK : (q + 1) * BLOCK]
            imag = both[DEVICES:, q * BLOCK : (q + 1) * BLOCK]
            if q == 0:
                c, s = cos, sin
            elif p == 0:
                c, s = own * cos + (1 - own) * sin, own * sin - (1 - own) * cos
            else:
                c, s = sin, -cos
            turned = jnp.concatenate(
                [(real * c - imag * s).astype(BF16), (real * s + imag * c).astype(BF16)], axis=1
            )
            parts.append(lax.dot_general(second[...], turned, NT, preferred_element_type=F32))
        if p == 0:
            low, high = parts[0] - (1 - own) * parts[1], (1 - own) * parts[0] + parts[1]
        else:
            low, high = parts[0] - parts[1], parts[0] + parts[1]
        for h in range(2):
            at = slice(h * BLOCK, (h + 1) * BLOCK)
            wide_out[pl.ds(h * ROWS + p, BLOCK, stride=2 * ROWS), :] = low[:, at]
            wide_out[pl.ds(h * ROWS + PAIRS + p, BLOCK, stride=2 * ROWS), :] = high[:, at]
    y[...] = wide_out[...].astype(BF16)


def length_transform(x, lone):
    vmem = pl.BlockSpec(memory_space=pltpu.VMEM)
    rows = DEVICES * ROWS
    return pl.pallas_call(
        length_body,
        in_specs=[pl.BlockSpec(memory_space=pltpu.SMEM), vmem, vmem, vmem, vmem],
        out_specs=vmem,
        out_shape=jax.ShapeDtypeStruct((rows, BLOCK), BF16),
        scratch_shapes=[pltpu.VMEM((rows, BLOCK), F32), pltpu.VMEM((rows, BLOCK), F32)],
        compiler_params=SMALL,
        name="length",
    )(
        lone,
        x,
        jnp.asarray(first_table(), BF16),
        jnp.asarray(twiddle(), F32),
        jnp.asarray(second_table(), BF16),
    )


def gate_body(normed, weight, out):
    logits = jnp.dot(normed[...], weight[...], preferred_element_type=F32)
    out[...] = jax.nn.sigmoid(logits)


def gate(normed, weight):
    steps = 8
    wide = D // steps
    return pl.pallas_call(
        gate_body,
        grid=(steps,),
        in_specs=[
            pl.BlockSpec((SEQS * BLOCK, D), lambda j: (0, 0)),
            pl.BlockSpec((D, wide), lambda j: (0, j)),
        ],
        out_specs=pl.BlockSpec((SEQS * BLOCK, wide), lambda j: (0, j)),
        out_shape=pltpu.VMEM((SEQS * BLOCK, D), F32),
        cost_estimate=pl.CostEstimate(
            flops=2 * SEQS * BLOCK * D * D, transcendentals=SEQS * BLOCK * D, bytes_accessed=2 * D * D
        ),
        compiler_params=SMALL,
        name="gate",
    )(in_hbm(normed), in_hbm(weight))


def leave_body(z, order, eye, weight, gates, out, matrix, spectral, gated, sems, arrive):
    wide = D // LEAVE
    loads = []
    for c in range(LEAVE):
        at = slice(c * wide, (c + 1) * wide)
        load = pltpu.make_async_copy(weight.at[:, at], matrix.at[:, at], arrive.at[c])
        load.start()
        loads.append(load)
    for s in range(SEQS):
        for g in range(GROUPS):
            rows = z[s * FW + g * GROUP_DIM : s * FW + (g + 1) * GROUP_DIM, :]
            turned = lax.dot_general(eye[...], rows, NT, preferred_element_type=F32)
            placed = jnp.dot(turned.astype(BF16), order[...], preferred_element_type=F32)
            spectral[s * BLOCK : (s + 1) * BLOCK, g * GROUP_DIM : (g + 1) * GROUP_DIM] = (
                placed.astype(BF16)
            )
    copies = []
    for c in range(LEAVE):
        at = slice(c * wide, (c + 1) * wide)
        loads[c].wait()
        mapped = jnp.dot(spectral[...], matrix[:, at], preferred_element_type=F32)
        block = (gates[:, at] * mapped).astype(BF16)
        for s in range(SEQS):
            gated[s, :, at] = block[s * BLOCK : (s + 1) * BLOCK]
        copy = pltpu.make_async_copy(gated.at[:, :, at], out.at[:, :, at], sems.at[c])
        copy.start()
        copies.append(copy)
    for copy in copies:
        copy.wait()


def leave(z, gates, weight):
    vmem = pl.BlockSpec(memory_space=pltpu.VMEM)
    hbm = pl.BlockSpec(memory_space=pltpu.HBM)
    return pl.pallas_call(
        leave_body,
        in_specs=[vmem, vmem, vmem, hbm, vmem],
        out_specs=hbm,
        out_shape=jax.ShapeDtypeStruct((SEQS, BLOCK, D), BF16),
        scratch_shapes=[
            pltpu.VMEM((FW, D), BF16),
            pltpu.VMEM((SEQS * BLOCK, FW), BF16),
            pltpu.VMEM((SEQS, BLOCK, D), BF16),
            pltpu.SemaphoreType.DMA((LEAVE,)),
            pltpu.SemaphoreType.DMA((LEAVE,)),
        ],
        compiler_params=SMALL,
        name="leave",
    )(z, jnp.asarray(channel_order(), BF16), jnp.asarray(np.eye(GROUP_DIM), BF16), in_hbm(weight), in_vmem(gates))


def exchange(x):
    return lax.all_to_all(x.reshape(DEVICES, ROWS, BLOCK), AXES, 0, 0, tiled=True).reshape(
        DEVICES * ROWS, BLOCK
    )


def local(tokens, norm_gain, mix_weight, gate_weight, out_weight):
    spectra, normed = enter(tokens, norm_gain, mix_weight)
    lone = (lax.axis_index(AXES) % (GROUP_DIM // ROWS) == 0).astype(F32).reshape(1)
    spectra, lone = lax.optimization_barrier((spectra, lone))
    arrived = exchange(spectra)
    gates = gate(normed, gate_weight)
    returned = exchange(length_transform(arrived, lone))
    return leave(returned, gates, out_weight)


def solution(mesh):
    return jax.shard_map(
        local,
        mesh=mesh,
        in_specs=(P(None, AXES, None), P(), P(), P(), P()),
        out_specs=P(None, AXES, None),
        check_vma=False,
    )
```

```python
import jax
import jax.numpy as jnp
import numpy as np
from jax import lax
from jax.experimental import pallas as pl
from jax.experimental.pallas import tpu as pltpu
from jax.sharding import PartitionSpec as P

AXES = ("row", "col")
DEVICES = 256
SEQS = 2
BLOCK = 128
D = 2048
GROUPS = 8
GROUP_DIM = 128
FW = GROUPS * GROUP_DIM
LENGTH = 32768
PAIRS = 4
ROWS = 2 * PAIRS
NT = (((1,), (1,)), ((), ()))
F32, BF16 = jnp.float32, jnp.bfloat16
LEAVE = 4
ENTER = 256
SMALL = pltpu.CompilerParams(vmem_limit_bytes=16 * 2**20)


def in_hbm(x):
    return pltpu.with_memory_space_constraint(x, pltpu.HBM)


def in_vmem(x):
    return pltpu.with_memory_space_constraint(x, pltpu.VMEM)


def group_table():
    table = np.zeros((GROUP_DIM, GROUP_DIM))
    j = np.arange(GROUP_DIM)
    for i in range(GROUP_DIM // ROWS):
        for p in range(PAIRS):
            k = PAIRS * i + p
            table[i * ROWS + p] = np.cos(2 * np.pi * j * k / GROUP_DIM)
            table[i * ROWS + PAIRS + p] = np.sin(2 * np.pi * j * k / GROUP_DIM)
    table[PAIRS] = np.cos(np.pi * j)
    return table / 8


def channel_order():
    order = np.zeros((GROUP_DIM, GROUP_DIM))
    for i in range(GROUP_DIM // ROWS):
        for p in range(PAIRS):
            k = PAIRS * i + p
            order[i * ROWS + p, k] = 1
            order[i * ROWS + PAIRS + p, (GROUP_DIM - k) if k else GROUP_DIM // 2] = 1
    return order


def first_table():
    m, d = np.arange(DEVICES)[:, None], np.arange(DEVICES)[None, :]
    angle = 2 * np.pi * (m * d % DEVICES) / DEVICES
    return np.concatenate([np.cos(angle), np.sin(angle)], axis=0) / 16


def twiddle():
    m, l = np.arange(DEVICES)[:, None], np.arange(BLOCK)[None, :]
    angle = 2 * np.pi * (m * l) / LENGTH
    return np.stack([np.cos(angle), np.sin(angle)])


def second_table():
    m, l = np.arange(BLOCK)[:, None], np.arange(BLOCK)[None, :]
    angle = 2 * np.pi * (m * l % BLOCK) / BLOCK
    return np.concatenate([np.cos(angle), -np.sin(angle)], axis=1) / 16


def enter_body(tokens, gain, weight, table, out, saved, held, scale, turn, normed, matrix, sems):
    def load(source, target, at):
        copy = pltpu.make_async_copy(source, target, sems.at[at])
        copy.start()
        return copy

    small = [load(gain, scale, 0), load(table, turn, 1)]
    rows_in = [load(tokens.at[s], held.at[s], 2 + s) for s in range(SEQS)]
    cuts = [slice(c * ENTER, (c + 1) * ENTER) for c in range(FW // ENTER)]
    chunks = [load(weight.at[:, cut], matrix.at[:, cut], 4 + c) for c, cut in enumerate(cuts)]
    for copy in small:
        copy.wait()
    for s in range(SEQS):
        rows_in[s].wait()

        def rows(i, _):
            at = pl.ds(pl.multiple_of(i * 16, 16), 16)
            t = held[s, at, :].astype(F32)
            inv = lax.rsqrt(jnp.mean(t * t, axis=-1, keepdims=True) + 1e-6)
            to = pl.ds(pl.multiple_of(s * BLOCK + i * 16, 16), 16)
            normed[to, :] = (t * inv * scale[...]).astype(BF16)
            return 0

        lax.fori_loop(0, BLOCK // 16, rows, 0, unroll=4)
    save = load(normed, saved, 4 + len(cuts))
    for chunk, cut in zip(chunks, cuts):
        chunk.wait()
        mixed = jnp.dot(normed[...], matrix[:, cut], preferred_element_type=F32).astype(BF16)
        for q in range(ENTER // GROUP_DIM):
            turned = lax.dot_general(
                turn[...],
                mixed[:, q * GROUP_DIM : (q + 1) * GROUP_DIM],
                NT,
                preferred_element_type=F32,
            )
            at = slice(cut.start + q * GROUP_DIM, cut.start + (q + 1) * GROUP_DIM)
            for s in range(SEQS):
                out[s, at, :] = turned[:, s * BLOCK : (s + 1) * BLOCK].astype(BF16)
    save.wait()


def enter(tokens, gain, weight):
    vmem = pl.BlockSpec(memory_space=pltpu.VMEM)
    hbm = pl.BlockSpec(memory_space=pltpu.HBM)
    return pl.pallas_call(
        enter_body,
        in_specs=[hbm] * 4,
        out_specs=[vmem, hbm],
        out_shape=[
            jax.ShapeDtypeStruct((SEQS, FW, BLOCK), BF16),
            pltpu.HBM((SEQS * BLOCK, D), BF16),
        ],
        scratch_shapes=[
            pltpu.VMEM((SEQS, BLOCK, D), BF16),
            pltpu.VMEM((1, D), F32),
            pltpu.VMEM((GROUP_DIM, GROUP_DIM), BF16),
            pltpu.VMEM((SEQS * BLOCK, D), BF16),
            pltpu.VMEM((D, FW), BF16),
            pltpu.SemaphoreType.DMA((5 + FW // ENTER,)),
        ],
        compiler_params=SMALL,
        name="enter",
    )(
        in_hbm(tokens),
        in_hbm(gain.reshape(1, D)),
        in_hbm(weight),
        in_hbm(jnp.asarray(group_table(), BF16)),
    )


def length_body(lone, x, first, twist, second, later, y, kept, wide_in, wide_out, sem):
    load = pltpu.make_async_copy(later, kept, sem)
    load.start()

    @pl.when(lone[0] >= 0)
    def _():
        over_positions(lone[0], x, first, twist, second, y, wide_in, wide_out)

    load.wait()


def over_positions(own, x, first, twist, second, y, wide_in, wide_out):
    wide_in[...] = x[...].astype(F32)
    cos, sin = twist[0], twist[1]
    for p in range(PAIRS):
        pair = jnp.concatenate(
            [
                wide_in[pl.ds(p, DEVICES, stride=ROWS), :].astype(BF16),
                wide_in[pl.ds(PAIRS + p, DEVICES, stride=ROWS), :].astype(BF16),
            ],
            axis=1,
        )
        both = jnp.dot(first[...], pair, preferred_element_type=F32)
        parts = []
        for q in range(2):
            real = both[:DEVICES, q * BLOCK : (q + 1) * BLOCK]
            imag = both[DEVICES:, q * BLOCK : (q + 1) * BLOCK]
            if q == 0:
                c, s = cos, sin
            elif p == 0:
                c, s = own * cos + (1 - own) * sin, own * sin - (1 - own) * cos
            else:
                c, s = sin, -cos
            turned = jnp.concatenate(
                [(real * c - imag * s).astype(BF16), (real * s + imag * c).astype(BF16)], axis=1
            )
            parts.append(lax.dot_general(second[...], turned, NT, preferred_element_type=F32))
        if p == 0:
            low, high = parts[0] - (1 - own) * parts[1], (1 - own) * parts[0] + parts[1]
        else:
            low, high = parts[0] - parts[1], parts[0] + parts[1]
        for h in range(2):
            at = slice(h * BLOCK, (h + 1) * BLOCK)
            wide_out[pl.ds(h * ROWS + p, BLOCK, stride=2 * ROWS), :] = low[:, at]
            wide_out[pl.ds(h * ROWS + PAIRS + p, BLOCK, stride=2 * ROWS), :] = high[:, at]
    y[...] = wide_out[...].astype(BF16)


def length_transform(x, lone, later):
    vmem = pl.BlockSpec(memory_space=pltpu.VMEM)
    rows = DEVICES * ROWS
    return pl.pallas_call(
        length_body,
        in_specs=[
            pl.BlockSpec(memory_space=pltpu.SMEM),
            vmem,
            vmem,
            vmem,
            vmem,
            pl.BlockSpec(memory_space=pltpu.HBM),
        ],
        out_specs=[vmem, vmem],
        out_shape=[jax.ShapeDtypeStruct((rows, BLOCK), BF16), pltpu.VMEM(later.shape, BF16)],
        scratch_shapes=[
            pltpu.VMEM((rows, BLOCK), F32),
            pltpu.VMEM((rows, BLOCK), F32),
            pltpu.SemaphoreType.DMA,
        ],
        compiler_params=SMALL,
        name="length",
    )(
        lone,
        x,
        jnp.asarray(first_table(), BF16),
        jnp.asarray(twiddle(), F32),
        jnp.asarray(second_table(), BF16),
        in_hbm(later),
    )


def gate_body(normed, weight, out):
    logits = jnp.dot(normed[...], weight[...], preferred_element_type=F32)
    out[...] = jax.nn.sigmoid(logits)


def gate(normed, weight):
    steps = 8
    wide = D // steps
    return pl.pallas_call(
        gate_body,
        grid=(steps,),
        in_specs=[
            pl.BlockSpec((SEQS * BLOCK, D), lambda j: (0, 0)),
            pl.BlockSpec((D, wide), lambda j: (0, j)),
        ],
        out_specs=pl.BlockSpec((SEQS * BLOCK, wide), lambda j: (0, j)),
        out_shape=pltpu.VMEM((SEQS * BLOCK, D), F32),
        cost_estimate=pl.CostEstimate(
            flops=2 * SEQS * BLOCK * D * D, transcendentals=SEQS * BLOCK * D, bytes_accessed=2 * D * D
        ),
        compiler_params=SMALL,
        name="gate",
    )(in_hbm(normed), in_hbm(weight))


def leave_body(z, order, eye, weight, gates, out, spectral, gated, sems):
    two = 2 * GROUP_DIM
    for g in range(FW // two):
        turned = [
            lax.dot_general(
                eye[...],
                z[s * FW + g * two : s * FW + (g + 1) * two, :],
                NT,
                preferred_element_type=F32,
            ).astype(BF16)
            for s in range(SEQS)
        ]
        placed = jnp.dot(jnp.concatenate(turned, axis=0), order[...], preferred_element_type=F32)
        spectral[:, g * two : (g + 1) * two] = placed.astype(BF16)
    copies = []
    wide = D // LEAVE
    for c in range(LEAVE):
        at = slice(c * wide, (c + 1) * wide)
        mapped = jnp.dot(spectral[...], weight[:, at], preferred_element_type=F32)
        block = (gates[:, at] * mapped).astype(BF16)
        for s in range(SEQS):
            gated[s, :, at] = block[s * BLOCK : (s + 1) * BLOCK]
        copy = pltpu.make_async_copy(gated.at[:, :, at], out.at[:, :, at], sems.at[c])
        copy.start()
        copies.append(copy)
    for copy in copies:
        copy.wait()


def leave(z, gates, weight):
    vmem = pl.BlockSpec(memory_space=pltpu.VMEM)
    return pl.pallas_call(
        leave_body,
        in_specs=[vmem] * 5,
        out_specs=pl.BlockSpec(memory_space=pltpu.HBM),
        out_shape=jax.ShapeDtypeStruct((SEQS, BLOCK, D), BF16),
        scratch_shapes=[
            pltpu.VMEM((SEQS * BLOCK, FW), BF16),
            pltpu.VMEM((SEQS, BLOCK, D), BF16),
            pltpu.SemaphoreType.DMA((LEAVE,)),
        ],
        compiler_params=SMALL,
        name="leave",
    )(
        z,
        jnp.asarray(np.kron(np.eye(2), channel_order()), BF16),
        jnp.asarray(np.eye(GROUP_DIM), BF16),
        in_vmem(weight),
        in_vmem(gates),
    )


def exchange(x):
    return lax.all_to_all(x.reshape(DEVICES, ROWS, BLOCK), AXES, 0, 0, tiled=True).reshape(
        DEVICES * ROWS, BLOCK
    )


def local(tokens, norm_gain, mix_weight, gate_weight, out_weight):
    spectra, normed = enter(tokens, norm_gain, mix_weight)
    lone = (lax.axis_index(AXES) % (GROUP_DIM // ROWS) == 0).astype(F32).reshape(1)
    arrived = exchange(spectra)
    arrived, gates = lax.optimization_barrier((arrived, gate(normed, gate_weight)))
    turned, matrix = length_transform(arrived, lone, out_weight)
    return leave(exchange(turned), gates, matrix)


def solution(mesh):
    return jax.shard_map(
        local,
        mesh=mesh,
        in_specs=(P(None, AXES, None), P(), P(), P(), P()),
        out_specs=P(None, AXES, None),
        check_vma=False,
    )
```

```python
import jax
import jax.numpy as jnp
import numpy as np
from jax import lax
from jax.experimental import pallas as pl
from jax.experimental.pallas import tpu as pltpu
from jax.sharding import PartitionSpec as P

AXES = ("row", "col")
DEVICES = 256
SEQS = 2
BLOCK = 128
D = 2048
GROUPS = 8
GROUP_DIM = 128
FW = GROUPS * GROUP_DIM
TWO = 2 * GROUP_DIM
LENGTH = 32768
PAIRS = 4
ROWS = 2 * PAIRS
NT = (((1,), (1,)), ((), ()))
F32, BF16 = jnp.float32, jnp.bfloat16
LEAVE = 4
EARLY = 1024
ENTER = 512
SMALL = pltpu.CompilerParams(vmem_limit_bytes=16 * 2**20)


def in_hbm(x):
    return pltpu.with_memory_space_constraint(x, pltpu.HBM)


def in_vmem(x):
    return pltpu.with_memory_space_constraint(x, pltpu.VMEM)


def group_table():
    table = np.zeros((GROUP_DIM, GROUP_DIM))
    j = np.arange(GROUP_DIM)
    for i in range(GROUP_DIM // ROWS):
        for p in range(PAIRS):
            k = PAIRS * i + p
            table[i * ROWS + p] = np.cos(2 * np.pi * j * k / GROUP_DIM)
            table[i * ROWS + PAIRS + p] = np.sin(2 * np.pi * j * k / GROUP_DIM)
    table[PAIRS] = np.cos(np.pi * j)
    return table / 8


def channel_order():
    order = np.zeros((GROUP_DIM, GROUP_DIM))
    for i in range(GROUP_DIM // ROWS):
        for p in range(PAIRS):
            k = PAIRS * i + p
            order[i * ROWS + p, k] = 1
            order[i * ROWS + PAIRS + p, (GROUP_DIM - k) if k else GROUP_DIM // 2] = 1
    return order


def first_table():
    m, d = np.arange(DEVICES)[:, None], np.arange(DEVICES)[None, :]
    angle = 2 * np.pi * (m * d % DEVICES) / DEVICES
    return np.concatenate([np.cos(angle), np.sin(angle)], axis=0) / 16


def twiddle():
    m, l = np.arange(DEVICES)[:, None], np.arange(BLOCK)[None, :]
    angle = 2 * np.pi * (m * l) / LENGTH
    return np.stack([np.cos(angle), np.sin(angle)])


def second_table():
    m, l = np.arange(BLOCK)[:, None], np.arange(BLOCK)[None, :]
    angle = 2 * np.pi * (m * l % BLOCK) / BLOCK
    return np.concatenate([np.cos(angle), -np.sin(angle)], axis=1) / 16


def enter_body(tokens, gain, weight, table, out, saved, held, scale, turn, normed, matrix, sems):
    def load(source, target, at):
        copy = pltpu.make_async_copy(source, target, sems.at[at])
        copy.start()
        return copy

    small = [load(gain, scale, 0), load(table, turn, 1)]
    rows_in = [load(tokens.at[s], held.at[s], 2 + s) for s in range(SEQS)]
    cuts = [slice(c * ENTER, (c + 1) * ENTER) for c in range(FW // ENTER)]
    chunks = [load(weight.at[:, cut], matrix.at[:, cut], 4 + c) for c, cut in enumerate(cuts)]
    for copy in small:
        copy.wait()
    for s in range(SEQS):
        rows_in[s].wait()

        def rows(i, _):
            at = pl.ds(pl.multiple_of(i * 16, 16), 16)
            t = held[s, at, :].astype(F32)
            inv = lax.rsqrt(jnp.mean(t * t, axis=-1, keepdims=True) + 1e-6)
            to = pl.ds(pl.multiple_of(s * BLOCK + i * 16, 16), 16)
            normed[to, :] = (t * inv * scale[...]).astype(BF16)
            return 0

        lax.fori_loop(0, BLOCK // 16, rows, 0, unroll=8)
    save = load(normed, saved, 4 + len(cuts))
    for chunk, cut in zip(chunks, cuts):
        chunk.wait()
        mixed = jnp.dot(normed[...], matrix[:, cut], preferred_element_type=F32).astype(BF16)
        for q in range(ENTER // TWO):
            part = mixed[:, q * TWO : (q + 1) * TWO]
            turned = lax.dot_general(turn[...], part, NT, preferred_element_type=F32)
            at = slice(cut.start + q * TWO, cut.start + (q + 1) * TWO)
            for s in range(SEQS):
                out[s, at, :] = turned[:, s * BLOCK : (s + 1) * BLOCK].astype(BF16)
    save.wait()


def enter(tokens, gain, weight):
    vmem = pl.BlockSpec(memory_space=pltpu.VMEM)
    hbm = pl.BlockSpec(memory_space=pltpu.HBM)
    return pl.pallas_call(
        enter_body,
        in_specs=[hbm] * 4,
        out_specs=[vmem, hbm],
        out_shape=[
            jax.ShapeDtypeStruct((SEQS, FW, BLOCK), BF16),
            pltpu.HBM((SEQS * BLOCK, D), BF16),
        ],
        scratch_shapes=[
            pltpu.VMEM((SEQS, BLOCK, D), BF16),
            pltpu.VMEM((1, D), F32),
            pltpu.VMEM((TWO, TWO), BF16),
            pltpu.VMEM((SEQS * BLOCK, D), BF16),
            pltpu.VMEM((D, FW), BF16),
            pltpu.SemaphoreType.DMA((5 + FW // ENTER,)),
        ],
        compiler_params=SMALL,
        name="enter",
    )(
        in_hbm(tokens),
        in_hbm(gain.reshape(1, D)),
        in_hbm(weight),
        in_hbm(jnp.asarray(np.kron(np.eye(2), group_table()), BF16)),
    )


def length_body(lone, x, first, twist, second, later, y, kept, wide_in, wide_out, sem):
    load = pltpu.make_async_copy(later.at[:, :EARLY], kept, sem)
    load.start()

    @pl.when(lone[0] >= 0)
    def _():
        over_positions(lone[0], x, first, twist, second, y, wide_in, wide_out)

    load.wait()


def over_positions(own, x, first, twist, second, y, wide_in, wide_out):
    wide_in[...] = x[...].astype(F32)
    cos, sin = twist[0], twist[1]
    for p in range(PAIRS):
        pair = jnp.concatenate(
            [
                wide_in[pl.ds(p, DEVICES, stride=ROWS), :].astype(BF16),
                wide_in[pl.ds(PAIRS + p, DEVICES, stride=ROWS), :].astype(BF16),
            ],
            axis=1,
        )
        both = jnp.dot(first[...], pair, preferred_element_type=F32)
        parts = []
        for q in range(2):
            real = both[:DEVICES, q * BLOCK : (q + 1) * BLOCK]
            imag = both[DEVICES:, q * BLOCK : (q + 1) * BLOCK]
            if q == 0:
                c, s = cos, sin
            elif p == 0:
                c, s = own * cos + (1 - own) * sin, own * sin - (1 - own) * cos
            else:
                c, s = sin, -cos
            turned = jnp.concatenate(
                [(real * c - imag * s).astype(BF16), (real * s + imag * c).astype(BF16)], axis=1
            )
            parts.append(lax.dot_general(second[...], turned, NT, preferred_element_type=F32))
        if p == 0:
            low, high = parts[0] - (1 - own) * parts[1], (1 - own) * parts[0] + parts[1]
        else:
            low, high = parts[0] - parts[1], parts[0] + parts[1]
        for h in range(2):
            at = slice(h * BLOCK, (h + 1) * BLOCK)
            wide_out[pl.ds(h * ROWS + p, BLOCK, stride=2 * ROWS), :] = low[:, at]
            wide_out[pl.ds(h * ROWS + PAIRS + p, BLOCK, stride=2 * ROWS), :] = high[:, at]
    y[...] = wide_out[...].astype(BF16)


def length_transform(x, lone, later):
    vmem = pl.BlockSpec(memory_space=pltpu.VMEM)
    rows = DEVICES * ROWS
    return pl.pallas_call(
        length_body,
        in_specs=[
            pl.BlockSpec(memory_space=pltpu.SMEM),
            vmem,
            vmem,
            vmem,
            vmem,
            pl.BlockSpec(memory_space=pltpu.HBM),
        ],
        out_specs=[vmem, vmem],
        out_shape=[jax.ShapeDtypeStruct((rows, BLOCK), BF16), pltpu.VMEM((FW, EARLY), BF16)],
        scratch_shapes=[
            pltpu.VMEM((rows, BLOCK), F32),
            pltpu.VMEM((rows, BLOCK), F32),
            pltpu.SemaphoreType.DMA,
        ],
        compiler_params=SMALL,
        name="length",
    )(
        lone,
        x,
        jnp.asarray(first_table(), BF16),
        jnp.asarray(twiddle(), F32),
        jnp.asarray(second_table(), BF16),
        in_hbm(later),
    )


def gate_body(normed, weight, out):
    logits = jnp.dot(normed[...], weight[...], preferred_element_type=F32)
    out[...] = jax.nn.sigmoid(logits)


def gate(normed, weight):
    steps = 8
    wide = D // steps
    return pl.pallas_call(
        gate_body,
        grid=(steps,),
        in_specs=[
            pl.BlockSpec((SEQS * BLOCK, D), lambda j: (0, 0)),
            pl.BlockSpec((D, wide), lambda j: (0, j)),
        ],
        out_specs=pl.BlockSpec((SEQS * BLOCK, wide), lambda j: (0, j)),
        out_shape=pltpu.VMEM((SEQS * BLOCK, D), F32),
        cost_estimate=pl.CostEstimate(
            flops=2 * SEQS * BLOCK * D * D, transcendentals=SEQS * BLOCK * D, bytes_accessed=2 * D * D
        ),
        compiler_params=SMALL,
        name="gate",
    )(in_hbm(normed), in_hbm(weight))


def leave_body(z, order, eye, early, weight, gates, out, late, spectral, gated, loaded, sems):
    wide = D // LEAVE
    loads = []
    for c in range(EARLY // wide, LEAVE):
        source = weight.at[:, c * wide : (c + 1) * wide]
        target = late.at[:, c * wide - EARLY : (c + 1) * wide - EARLY]
        loads.append(pltpu.make_async_copy(source, target, loaded.at[c - EARLY // wide]))
        loads[-1].start()

    def reorder(g, _):
        for h in range(2):
            at = pl.multiple_of((2 * g + h) * TWO, TWO)
            turned = [
                lax.dot_general(
                    eye[...],
                    z[pl.ds(pl.multiple_of(s * FW + at, TWO), TWO), :],
                    NT,
                    preferred_element_type=F32,
                ).astype(BF16)
                for s in range(SEQS)
            ]
            placed = jnp.dot(
                jnp.concatenate(turned, axis=0), order[...], preferred_element_type=F32
            )
            spectral[:, pl.ds(at, TWO)] = placed.astype(BF16)
        return 0

    lax.fori_loop(0, FW // TWO // 2, reorder, 0)
    copies = []
    for c in range(LEAVE):
        at = slice(c * wide, (c + 1) * wide)
        if c * wide < EARLY:
            part = early[:, at]
        else:
            loads[c - EARLY // wide].wait()
            part = late[:, c * wide - EARLY : (c + 1) * wide - EARLY]
        mapped = jnp.dot(spectral[...], part, preferred_element_type=F32)
        block = (gates[:, at] * mapped).astype(BF16)
        for s in range(SEQS):
            gated[s, :, at] = block[s * BLOCK : (s + 1) * BLOCK]
        copy = pltpu.make_async_copy(gated.at[:, :, at], out.at[:, :, at], sems.at[c])
        copy.start()
        copies.append(copy)
    for copy in copies:
        copy.wait()


def leave(z, gates, early, weight):
    vmem = pl.BlockSpec(memory_space=pltpu.VMEM)
    hbm = pl.BlockSpec(memory_space=pltpu.HBM)
    return pl.pallas_call(
        leave_body,
        in_specs=[vmem, vmem, vmem, vmem, hbm, vmem],
        out_specs=hbm,
        out_shape=jax.ShapeDtypeStruct((SEQS, BLOCK, D), BF16),
        scratch_shapes=[
            pltpu.VMEM((FW, D - EARLY), BF16),
            pltpu.VMEM((SEQS * BLOCK, FW), BF16),
            pltpu.VMEM((SEQS, BLOCK, D), BF16),
            pltpu.SemaphoreType.DMA((LEAVE,)),
            pltpu.SemaphoreType.DMA((LEAVE,)),
        ],
        compiler_params=SMALL,
        name="leave",
    )(
        z,
        jnp.asarray(np.kron(np.eye(2), channel_order()), BF16),
        jnp.asarray(np.eye(GROUP_DIM), BF16),
        in_vmem(early),
        in_hbm(weight),
        in_vmem(gates),
    )


def exchange(x):
    return lax.all_to_all(x.reshape(DEVICES, ROWS, BLOCK), AXES, 0, 0, tiled=True).reshape(
        DEVICES * ROWS, BLOCK
    )


def local(tokens, norm_gain, mix_weight, gate_weight, out_weight):
    spectra, normed = enter(tokens, norm_gain, mix_weight)
    lone = (lax.axis_index(AXES) % (GROUP_DIM // ROWS) == 0).astype(F32).reshape(1)
    arrived = exchange(spectra)
    arrived, gates = lax.optimization_barrier((arrived, gate(normed, gate_weight)))
    turned, early = length_transform(arrived, lone, out_weight)
    return leave(exchange(turned), gates, early, out_weight)


def solution(mesh):
    return jax.shard_map(
        local,
        mesh=mesh,
        in_specs=(P(None, AXES, None), P(), P(), P(), P()),
        out_specs=P(None, AXES, None),
        check_vma=False,
    )
```

```python
import jax
import jax.numpy as jnp
import numpy as np
from jax import lax
from jax.experimental import pallas as pl
from jax.experimental.pallas import tpu as pltpu
from jax.sharding import PartitionSpec as P

AXES = ("row", "col")
DEVICES = 256
SEQS = 2
BLOCK = 128
D = 2048
LEAVE = 4
PARTS = D // LEAVE
GROUPS = 8
GROUP_DIM = 128
FW = GROUPS * GROUP_DIM
TWO = 2 * GROUP_DIM
LENGTH = 32768
PAIRS = 4
ROWS = 2 * PAIRS
NT = (((1,), (1,)), ((), ()))
F32, BF16 = jnp.float32, jnp.bfloat16
ENTER = 512
SMALL = pltpu.CompilerParams(vmem_limit_bytes=16 * 2**20)


def in_hbm(x):
    return pltpu.with_memory_space_constraint(x, pltpu.HBM)


def in_vmem(x):
    return pltpu.with_memory_space_constraint(x, pltpu.VMEM)


def group_table():
    table = np.zeros((GROUP_DIM, GROUP_DIM))
    j = np.arange(GROUP_DIM)
    for i in range(GROUP_DIM // ROWS):
        for p in range(PAIRS):
            k = PAIRS * i + p
            table[i * ROWS + p] = np.cos(2 * np.pi * j * k / GROUP_DIM)
            table[i * ROWS + PAIRS + p] = np.sin(2 * np.pi * j * k / GROUP_DIM)
    table[PAIRS] = np.cos(np.pi * j)
    return table / 8


def channel_order():
    order = np.zeros((GROUP_DIM, GROUP_DIM))
    for i in range(GROUP_DIM // ROWS):
        for p in range(PAIRS):
            k = PAIRS * i + p
            order[i * ROWS + p, k] = 1
            order[i * ROWS + PAIRS + p, (GROUP_DIM - k) if k else GROUP_DIM // 2] = 1
    return order


def first_table():
    m, d = np.arange(DEVICES)[:, None], np.arange(DEVICES)[None, :]
    angle = 2 * np.pi * (m * d % DEVICES) / DEVICES
    return np.concatenate([np.cos(angle), np.sin(angle)], axis=0) / 16


def twiddle():
    m, l = np.arange(DEVICES)[:, None], np.arange(BLOCK)[None, :]
    angle = 2 * np.pi * (m * l) / LENGTH
    return np.stack([np.cos(angle), np.sin(angle)])


def second_table():
    m, l = np.arange(BLOCK)[:, None], np.arange(BLOCK)[None, :]
    angle = 2 * np.pi * (m * l % BLOCK) / BLOCK
    return np.concatenate([np.cos(angle), -np.sin(angle)], axis=1) / 16


def enter_body(
    tokens, gain, weight, table, out, saved, held, scale, turn, normed, matrix, spectra, sems
):
    def load(source, target, at):
        copy = pltpu.make_async_copy(source, target, sems.at[at])
        copy.start()
        return copy

    small = [load(gain, scale, 0), load(table, turn, 1)]
    rows_in = [load(tokens.at[s], held.at[s], 2 + s) for s in range(SEQS)]
    cuts = [slice(c * ENTER, (c + 1) * ENTER) for c in range(FW // ENTER)]
    chunks = [load(weight.at[:, cut], matrix.at[:, cut], 4 + c) for c, cut in enumerate(cuts)]
    for copy in small:
        copy.wait()
    for s in range(SEQS):
        rows_in[s].wait()

        def rows(i, _):
            at = pl.ds(pl.multiple_of(i * 16, 16), 16)
            t = held[s, at, :].astype(F32)
            inv = lax.rsqrt(jnp.mean(t * t, axis=-1, keepdims=True) + 1e-6)
            to = pl.ds(pl.multiple_of(s * BLOCK + i * 16, 16), 16)
            normed[to, :] = (t * inv * scale[...]).astype(BF16)
            return 0

        lax.fori_loop(0, BLOCK // 16, rows, 0, unroll=8)
    saves = [load(normed, saved, 4 + len(cuts))]
    for chunk, cut in zip(chunks, cuts):
        chunk.wait()
        mixed = jnp.dot(normed[...], matrix[:, cut], preferred_element_type=F32).astype(BF16)
        for q in range(ENTER // TWO):
            part = mixed[:, q * TWO : (q + 1) * TWO]
            turned = lax.dot_general(turn[...], part, NT, preferred_element_type=F32)
            at = slice(cut.start + q * TWO, cut.start + (q + 1) * TWO)
            for s in range(SEQS):
                spectra[s, at, :] = turned[:, s * BLOCK : (s + 1) * BLOCK].astype(BF16)
        saves.append(load(spectra.at[:, cut], out.at[:, cut], 4 + len(cuts) + len(saves)))
    for save in saves:
        save.wait()


def enter(tokens, gain, weight):
    hbm = pl.BlockSpec(memory_space=pltpu.HBM)
    return pl.pallas_call(
        enter_body,
        in_specs=[hbm] * 4,
        out_specs=[hbm, hbm],
        out_shape=[
            pltpu.HBM((SEQS, FW, BLOCK), BF16),
            pltpu.HBM((SEQS * BLOCK, D), BF16),
        ],
        scratch_shapes=[
            pltpu.VMEM((SEQS, BLOCK, D), BF16),
            pltpu.VMEM((1, D), F32),
            pltpu.VMEM((TWO, TWO), BF16),
            pltpu.VMEM((SEQS * BLOCK, D), BF16),
            pltpu.VMEM((D, FW), BF16),
            pltpu.VMEM((SEQS, FW, BLOCK), BF16),
            pltpu.SemaphoreType.DMA((5 + 2 * (FW // ENTER),)),
        ],
        compiler_params=SMALL,
        name="enter",
    )(
        in_hbm(tokens),
        in_hbm(gain.reshape(1, D)),
        in_hbm(weight),
        in_hbm(jnp.asarray(np.kron(np.eye(2), group_table()), BF16)),
    )


def length_body(lone, x, first, twist, second, later, y, kept, wide_in, wide_out, sem):
    load = pltpu.make_async_copy(later.at[:, PARTS : 2 * PARTS], kept, sem)
    load.start()

    @pl.when(lone[0] >= 0)
    def _():
        over_positions(lone[0], x, first, twist, second, y, wide_in, wide_out)

    load.wait()


def over_positions(own, x, first, twist, second, y, wide_in, wide_out):
    wide_in[...] = x[...].astype(F32)
    cos, sin = twist[0], twist[1]
    for p in range(PAIRS):
        pair = jnp.concatenate(
            [
                wide_in[pl.ds(p, DEVICES, stride=ROWS), :].astype(BF16),
                wide_in[pl.ds(PAIRS + p, DEVICES, stride=ROWS), :].astype(BF16),
            ],
            axis=1,
        )
        both = jnp.dot(first[...], pair, preferred_element_type=F32)
        parts = []
        for q in range(2):
            real = both[:DEVICES, q * BLOCK : (q + 1) * BLOCK]
            imag = both[DEVICES:, q * BLOCK : (q + 1) * BLOCK]
            if q == 0:
                c, s = cos, sin
            elif p == 0:
                c, s = own * cos + (1 - own) * sin, own * sin - (1 - own) * cos
            else:
                c, s = sin, -cos
            turned = jnp.concatenate(
                [(real * c - imag * s).astype(BF16), (real * s + imag * c).astype(BF16)], axis=1
            )
            parts.append(lax.dot_general(second[...], turned, NT, preferred_element_type=F32))
        if p == 0:
            low, high = parts[0] - (1 - own) * parts[1], (1 - own) * parts[0] + parts[1]
        else:
            low, high = parts[0] - parts[1], parts[0] + parts[1]
        for h in range(2):
            at = slice(h * BLOCK, (h + 1) * BLOCK)
            wide_out[pl.ds(h * ROWS + p, BLOCK, stride=2 * ROWS), :] = low[:, at]
            wide_out[pl.ds(h * ROWS + PAIRS + p, BLOCK, stride=2 * ROWS), :] = high[:, at]
    y[...] = wide_out[...].astype(BF16)


def length_transform(x, lone, later):
    vmem = pl.BlockSpec(memory_space=pltpu.VMEM)
    rows = DEVICES * ROWS
    return pl.pallas_call(
        length_body,
        in_specs=[
            pl.BlockSpec(memory_space=pltpu.SMEM),
            vmem,
            vmem,
            vmem,
            vmem,
            pl.BlockSpec(memory_space=pltpu.HBM),
        ],
        out_specs=[vmem, vmem],
        out_shape=[jax.ShapeDtypeStruct((rows, BLOCK), BF16), pltpu.VMEM((FW, PARTS), BF16)],
        scratch_shapes=[
            pltpu.VMEM((rows, BLOCK), F32),
            pltpu.VMEM((rows, BLOCK), F32),
            pltpu.SemaphoreType.DMA,
        ],
        compiler_params=SMALL,
        name="length",
    )(
        lone,
        x,
        jnp.asarray(first_table(), BF16),
        jnp.asarray(twiddle(), F32),
        jnp.asarray(second_table(), BF16),
        in_hbm(later),
    )


def gate_body(normed, weight, later, out, kept, sem):
    load = pltpu.make_async_copy(later.at[:, :PARTS], kept, sem)

    @pl.when(pl.program_id(0) == 0)
    def _():
        load.start()

    logits = jnp.dot(normed[...], weight[...], preferred_element_type=F32)
    out[...] = jax.nn.sigmoid(logits).astype(BF16)

    @pl.when(pl.program_id(0) == pl.num_programs(0) - 1)
    def _():
        load.wait()


def gate(normed, weight, later):
    steps = 8
    wide = D // steps
    return pl.pallas_call(
        gate_body,
        grid=(steps,),
        in_specs=[
            pl.BlockSpec((SEQS * BLOCK, D), lambda j: (0, 0)),
            pl.BlockSpec((D, wide), lambda j: (0, j)),
            pl.BlockSpec(memory_space=pltpu.HBM),
        ],
        out_specs=[
            pl.BlockSpec((SEQS * BLOCK, wide), lambda j: (0, j)),
            pl.BlockSpec(memory_space=pltpu.VMEM),
        ],
        out_shape=[pltpu.VMEM((SEQS * BLOCK, D), BF16), pltpu.VMEM((FW, PARTS), BF16)],
        scratch_shapes=[pltpu.SemaphoreType.DMA],
        cost_estimate=pl.CostEstimate(
            flops=2 * SEQS * BLOCK * D * D, transcendentals=SEQS * BLOCK * D, bytes_accessed=2 * D * D
        ),
        compiler_params=SMALL,
        name="gate",
    )(in_hbm(normed), in_hbm(weight), in_hbm(later))


def leave_body(
    lone, z, order, eye, part_0, part_1, weight, gates, out, late, spectral, gated, loaded, sems
):
    loads = []
    for c in range(2, LEAVE):
        source = weight.at[:, c * PARTS : (c + 1) * PARTS]
        loads.append(pltpu.make_async_copy(source, late.at[c - 2], loaded.at[c - 2]))
        loads[-1].start()

    @pl.when(lone[0] >= 0)
    def _():
        for g in range(FW // TWO):
            turned = [
                lax.dot_general(
                    eye[...],
                    z[s * FW + g * TWO : s * FW + (g + 1) * TWO, :],
                    NT,
                    preferred_element_type=F32,
                ).astype(BF16)
                for s in range(SEQS)
            ]
            placed = jnp.dot(
                jnp.concatenate(turned, axis=0), order[...], preferred_element_type=F32
            )
            spectral[:, g * TWO : (g + 1) * TWO] = placed.astype(BF16)

    copies = []
    for c in range(LEAVE):
        at = slice(c * PARTS, (c + 1) * PARTS)
        if c >= 2:
            loads[c - 2].wait()
        part = (part_0, part_1)[c][...] if c < 2 else late[c - 2]
        mapped = jnp.dot(spectral[...], part, preferred_element_type=F32)
        block = (gates[:, at].astype(F32) * mapped).astype(BF16)
        for s in range(SEQS):
            gated[s, :, at] = block[s * BLOCK : (s + 1) * BLOCK]
        copy = pltpu.make_async_copy(gated.at[:, :, at], out.at[:, :, at], sems.at[c])
        copy.start()
        copies.append(copy)
    for copy in copies:
        copy.wait()


def leave(z, gates, part_0, part_1, weight, lone):
    vmem = pl.BlockSpec(memory_space=pltpu.VMEM)
    hbm = pl.BlockSpec(memory_space=pltpu.HBM)
    return pl.pallas_call(
        leave_body,
        in_specs=[pl.BlockSpec(memory_space=pltpu.SMEM), vmem, vmem, vmem, vmem, vmem, hbm, vmem],
        out_specs=hbm,
        out_shape=jax.ShapeDtypeStruct((SEQS, BLOCK, D), BF16),
        scratch_shapes=[
            pltpu.VMEM((LEAVE - 2, FW, PARTS), BF16),
            pltpu.VMEM((SEQS * BLOCK, FW), BF16),
            pltpu.VMEM((SEQS, BLOCK, D), BF16),
            pltpu.SemaphoreType.DMA((LEAVE,)),
            pltpu.SemaphoreType.DMA((LEAVE,)),
        ],
        compiler_params=SMALL,
        name="leave",
    )(
        lone,
        z,
        jnp.asarray(np.kron(np.eye(2), channel_order()), BF16),
        jnp.asarray(np.eye(GROUP_DIM), BF16),
        in_vmem(part_0),
        in_vmem(part_1),
        in_hbm(weight),
        in_vmem(gates),
    )


def exchange(x):
    return lax.all_to_all(x.reshape(DEVICES, ROWS, BLOCK), AXES, 0, 0, tiled=True).reshape(
        DEVICES * ROWS, BLOCK
    )


def local(tokens, norm_gain, mix_weight, gate_weight, out_weight):
    spectra, normed = enter(tokens, norm_gain, mix_weight)
    lone = (lax.axis_index(AXES) % (GROUP_DIM // ROWS) == 0).astype(F32).reshape(1)
    arrived = exchange(spectra)
    arrived, (gates, part_0) = lax.optimization_barrier(
        (arrived, gate(normed, gate_weight, out_weight))
    )
    turned, part_1 = length_transform(arrived, lone, out_weight)
    return leave(exchange(turned), gates, part_0, part_1, out_weight, lone)


def solution(mesh):
    return jax.shard_map(
        local,
        mesh=mesh,
        in_specs=(P(None, AXES, None), P(), P(), P(), P()),
        out_specs=P(None, AXES, None),
        check_vma=False,
    )
```

```python
import jax
import jax.numpy as jnp
import numpy as np
from jax import lax
from jax.experimental import pallas as pl
from jax.experimental.pallas import tpu as pltpu
from jax.sharding import PartitionSpec as P

AXES = ("row", "col")
DEVICES = 256
SEQS = 2
BLOCK = 128
D = 2048
LEAVE = 4
PARTS = D // LEAVE
GROUPS = 8
GROUP_DIM = 128
FW = GROUPS * GROUP_DIM
TWO = 2 * GROUP_DIM
LENGTH = 32768
PAIRS = 4
ROWS = 2 * PAIRS
NT = (((1,), (1,)), ((), ()))
TN = (((0,), (0,)), ((), ()))
F32, BF16 = jnp.float32, jnp.bfloat16
ENTER = 512
SMALL = pltpu.CompilerParams(vmem_limit_bytes=16 * 2**20)


def in_hbm(x):
    return pltpu.with_memory_space_constraint(x, pltpu.HBM)


def in_vmem(x):
    return pltpu.with_memory_space_constraint(x, pltpu.VMEM)


def group_table():
    table = np.zeros((GROUP_DIM, GROUP_DIM))
    j = np.arange(GROUP_DIM)
    for i in range(GROUP_DIM // ROWS):
        for p in range(PAIRS):
            k = PAIRS * i + p
            table[i * ROWS + p] = np.cos(2 * np.pi * j * k / GROUP_DIM)
            table[i * ROWS + PAIRS + p] = np.sin(2 * np.pi * j * k / GROUP_DIM)
    table[PAIRS] = np.cos(np.pi * j)
    return table / 8


def channel_order():
    order = np.zeros((GROUP_DIM, GROUP_DIM))
    for i in range(GROUP_DIM // ROWS):
        for p in range(PAIRS):
            k = PAIRS * i + p
            order[i * ROWS + p, k] = 1
            order[i * ROWS + PAIRS + p, (GROUP_DIM - k) if k else GROUP_DIM // 2] = 1
    return order


def first_table():
    m, d = np.arange(DEVICES)[:, None], np.arange(DEVICES)[None, :]
    angle = 2 * np.pi * (m * d % DEVICES) / DEVICES
    return np.concatenate([np.cos(angle), np.sin(angle)], axis=0) / 16


def twiddle():
    m, l = np.arange(DEVICES)[:, None], np.arange(BLOCK)[None, :]
    angle = 2 * np.pi * (m * l) / LENGTH
    return np.stack([np.cos(angle), np.sin(angle)])


def second_table():
    m, l = np.arange(BLOCK)[:, None], np.arange(BLOCK)[None, :]
    angle = 2 * np.pi * (m * l % BLOCK) / BLOCK
    return np.concatenate([np.cos(angle), -np.sin(angle)], axis=1) / 16


def enter_body(
    tokens, gain, weight, table, out, saved, held, scale, turn, normed, matrix, spectra, sems
):
    def load(source, target, at):
        copy = pltpu.make_async_copy(source, target, sems.at[at])
        copy.start()
        return copy

    small = [load(gain, scale, 0), load(table, turn, 1)]
    rows_in = [load(tokens.at[s], held.at[s], 2 + s) for s in range(SEQS)]
    cuts = [slice(c * ENTER, (c + 1) * ENTER) for c in range(FW // ENTER)]
    chunks = [load(weight.at[:, cut], matrix.at[:, cut], 4 + c) for c, cut in enumerate(cuts)]
    for copy in small:
        copy.wait()
    for s in range(SEQS):
        rows_in[s].wait()

        def rows(i, _):
            at = pl.ds(pl.multiple_of(i * 16, 16), 16)
            t = held[s, at, :].astype(F32)
            inv = lax.rsqrt(jnp.mean(t * t, axis=-1, keepdims=True) + 1e-6)
            to = pl.ds(pl.multiple_of(s * BLOCK + i * 16, 16), 16)
            normed[to, :] = (t * inv * scale[...]).astype(BF16)
            return 0

        lax.fori_loop(0, BLOCK // 16, rows, 0, unroll=8)
    saves = []
    for chunk, cut in zip(chunks, cuts):
        chunk.wait()
        if cut.stop == FW:
            saves.append(load(normed, saved, 4 + len(cuts) + len(saves)))
        mixed = jnp.dot(normed[...], matrix[:, cut], preferred_element_type=F32).astype(BF16)
        for q in range(ENTER // TWO):
            part = mixed[:, q * TWO : (q + 1) * TWO]
            turned = lax.dot_general(turn[...], part, NT, preferred_element_type=F32)
            at = slice(cut.start + q * TWO, cut.start + (q + 1) * TWO)
            for s in range(SEQS):
                spectra[s, at, :] = turned[:, s * BLOCK : (s + 1) * BLOCK].astype(BF16)
        saves.append(load(spectra.at[:, cut], out.at[:, cut], 4 + len(cuts) + len(saves)))
    for save in saves:
        save.wait()


def enter(tokens, gain, weight):
    hbm = pl.BlockSpec(memory_space=pltpu.HBM)
    return pl.pallas_call(
        enter_body,
        in_specs=[hbm] * 4,
        out_specs=[hbm, hbm],
        out_shape=[
            pltpu.HBM((SEQS, FW, BLOCK), BF16),
            pltpu.HBM((SEQS * BLOCK, D), BF16),
        ],
        scratch_shapes=[
            pltpu.VMEM((SEQS, BLOCK, D), BF16),
            pltpu.VMEM((1, D), F32),
            pltpu.VMEM((TWO, TWO), BF16),
            pltpu.VMEM((SEQS * BLOCK, D), BF16),
            pltpu.VMEM((D, FW), BF16),
            pltpu.VMEM((SEQS, FW, BLOCK), BF16),
            pltpu.SemaphoreType.DMA((5 + 2 * (FW // ENTER),)),
        ],
        compiler_params=SMALL,
        name="enter",
    )(
        in_hbm(tokens),
        in_hbm(gain.reshape(1, D)),
        in_hbm(weight),
        in_hbm(jnp.asarray(np.kron(np.eye(2), group_table()), BF16)),
    )


def length_body(lone, x, first, twist, second, later, y, kept, wide_in, wide_out, sem):
    load = pltpu.make_async_copy(later.at[:, PARTS : 2 * PARTS], kept, sem)
    load.start()

    @pl.when(lone[0] >= 0)
    def _():
        over_positions(lone[0], x, first, twist, second, y, wide_in, wide_out)

    load.wait()


def over_positions(own, x, first, twist, second, y, wide_in, wide_out):
    wide_in[...] = x[...].astype(F32)
    cos, sin = twist[0], twist[1]
    for p in range(PAIRS):
        pair = jnp.concatenate(
            [
                wide_in[pl.ds(p, DEVICES, stride=ROWS), :].astype(BF16),
                wide_in[pl.ds(PAIRS + p, DEVICES, stride=ROWS), :].astype(BF16),
            ],
            axis=1,
        )
        both = jnp.dot(first[...], pair, preferred_element_type=F32)
        parts = []
        for q in range(2):
            real = both[:DEVICES, q * BLOCK : (q + 1) * BLOCK]
            imag = both[DEVICES:, q * BLOCK : (q + 1) * BLOCK]
            if q == 0:
                c, s = cos, sin
            elif p == 0:
                c, s = own * cos + (1 - own) * sin, own * sin - (1 - own) * cos
            else:
                c, s = sin, -cos
            turned = jnp.concatenate(
                [(real * c - imag * s).astype(BF16), (real * s + imag * c).astype(BF16)], axis=1
            )
            parts.append(lax.dot_general(second[...], turned, NT, preferred_element_type=F32))
        if p == 0:
            low, high = parts[0] - (1 - own) * parts[1], (1 - own) * parts[0] + parts[1]
        else:
            low, high = parts[0] - parts[1], parts[0] + parts[1]
        for h in range(2):
            at = slice(h * BLOCK, (h + 1) * BLOCK)
            wide_out[pl.ds(h * ROWS + p, BLOCK, stride=2 * ROWS), :] = low[:, at]
            wide_out[pl.ds(h * ROWS + PAIRS + p, BLOCK, stride=2 * ROWS), :] = high[:, at]
    y[...] = wide_out[...].astype(BF16)


def length_transform(x, lone, later):
    vmem = pl.BlockSpec(memory_space=pltpu.VMEM)
    rows = DEVICES * ROWS
    return pl.pallas_call(
        length_body,
        in_specs=[
            pl.BlockSpec(memory_space=pltpu.SMEM),
            vmem,
            vmem,
            vmem,
            vmem,
            pl.BlockSpec(memory_space=pltpu.HBM),
        ],
        out_specs=[vmem, vmem],
        out_shape=[jax.ShapeDtypeStruct((rows, BLOCK), BF16), pltpu.VMEM((FW, PARTS), BF16)],
        scratch_shapes=[
            pltpu.VMEM((rows, BLOCK), F32),
            pltpu.VMEM((rows, BLOCK), F32),
            pltpu.SemaphoreType.DMA,
        ],
        compiler_params=SMALL,
        name="length",
    )(
        lone,
        x,
        jnp.asarray(first_table(), BF16),
        jnp.asarray(twiddle(), F32),
        jnp.asarray(second_table(), BF16),
        in_hbm(later),
    )


def gate_body(normed, weight, later, out, kept, sem):
    load = pltpu.make_async_copy(later.at[:, :PARTS], kept, sem)

    @pl.when(pl.program_id(0) == 0)
    def _():
        load.start()

    logits = jnp.dot(normed[...], weight[...], preferred_element_type=F32)
    out[...] = jax.nn.sigmoid(logits).astype(BF16)

    @pl.when(pl.program_id(0) == pl.num_programs(0) - 1)
    def _():
        load.wait()


def gate(normed, weight, later):
    steps = 8
    wide = D // steps
    return pl.pallas_call(
        gate_body,
        grid=(steps,),
        in_specs=[
            pl.BlockSpec((SEQS * BLOCK, D), lambda j: (0, 0)),
            pl.BlockSpec((D, wide), lambda j: (0, j)),
            pl.BlockSpec(memory_space=pltpu.HBM),
        ],
        out_specs=[
            pl.BlockSpec((SEQS * BLOCK, wide), lambda j: (0, j)),
            pl.BlockSpec(memory_space=pltpu.VMEM),
        ],
        out_shape=[pltpu.VMEM((SEQS * BLOCK, D), BF16), pltpu.VMEM((FW, PARTS), BF16)],
        scratch_shapes=[pltpu.SemaphoreType.DMA],
        cost_estimate=pl.CostEstimate(
            flops=2 * SEQS * BLOCK * D * D, transcendentals=SEQS * BLOCK * D, bytes_accessed=2 * D * D
        ),
        compiler_params=SMALL,
        name="gate",
    )(in_hbm(normed), in_hbm(weight), in_hbm(later))


def leave_body(
    lone, z, order, part_0, part_1, weight, gates, out, late, spectral, gated, loaded, sems
):
    loads = []
    for c in range(2, LEAVE):
        source = weight.at[:, c * PARTS : (c + 1) * PARTS]
        loads.append(pltpu.make_async_copy(source, late.at[c - 2], loaded.at[c - 2]))
        loads[-1].start()

    @pl.when(lone[0] >= 0)
    def _():
        for g in range(FW // TWO):
            for s in range(SEQS):
                rows = z[s * FW + g * TWO : s * FW + (g + 1) * TWO, :]
                placed = lax.dot_general(rows, order[...], TN, preferred_element_type=F32)
                spectral[s * BLOCK : (s + 1) * BLOCK, g * TWO : (g + 1) * TWO] = placed.astype(BF16)

    copies = []
    for c in range(LEAVE):
        at = slice(c * PARTS, (c + 1) * PARTS)
        if c >= 2:
            loads[c - 2].wait()
        part = (part_0, part_1)[c][...] if c < 2 else late[c - 2]
        mapped = jnp.dot(spectral[...], part, preferred_element_type=F32)
        block = (gates[:, at].astype(F32) * mapped).astype(BF16)
        for s in range(SEQS):
            gated[s, :, at] = block[s * BLOCK : (s + 1) * BLOCK]
        copy = pltpu.make_async_copy(gated.at[:, :, at], out.at[:, :, at], sems.at[c])
        copy.start()
        copies.append(copy)
    for copy in copies:
        copy.wait()


def leave(z, gates, part_0, part_1, weight, lone):
    vmem = pl.BlockSpec(memory_space=pltpu.VMEM)
    hbm = pl.BlockSpec(memory_space=pltpu.HBM)
    return pl.pallas_call(
        leave_body,
        in_specs=[pl.BlockSpec(memory_space=pltpu.SMEM), vmem, vmem, vmem, vmem, hbm, vmem],
        out_specs=hbm,
        out_shape=jax.ShapeDtypeStruct((SEQS, BLOCK, D), BF16),
        scratch_shapes=[
            pltpu.VMEM((LEAVE - 2, FW, PARTS), BF16),
            pltpu.VMEM((SEQS * BLOCK, FW), BF16),
            pltpu.VMEM((SEQS, BLOCK, D), BF16),
            pltpu.SemaphoreType.DMA((LEAVE,)),
            pltpu.SemaphoreType.DMA((LEAVE,)),
        ],
        compiler_params=SMALL,
        name="leave",
    )(
        lone,
        z,
        jnp.asarray(np.kron(np.eye(2), channel_order()), BF16),
        in_vmem(part_0),
        in_vmem(part_1),
        in_hbm(weight),
        in_vmem(gates),
    )


def exchange(x):
    return lax.all_to_all(x.reshape(DEVICES, ROWS, BLOCK), AXES, 0, 0, tiled=True).reshape(
        DEVICES * ROWS, BLOCK
    )


def local(tokens, norm_gain, mix_weight, gate_weight, out_weight):
    spectra, normed = enter(tokens, norm_gain, mix_weight)
    lone = (lax.axis_index(AXES) % (GROUP_DIM // ROWS) == 0).astype(F32).reshape(1)
    arrived = exchange(spectra)
    arrived, (gates, part_0) = lax.optimization_barrier(
        (arrived, gate(normed, gate_weight, out_weight))
    )
    turned, part_1 = length_transform(arrived, lone, out_weight)
    return leave(exchange(turned), gates, part_0, part_1, out_weight, lone)


def solution(mesh):
    return jax.shard_map(
        local,
        mesh=mesh,
        in_specs=(P(None, AXES, None), P(), P(), P(), P()),
        out_specs=P(None, AXES, None),
        check_vma=False,
    )
```

```python
import jax
import jax.numpy as jnp
import numpy as np
from jax import lax
from jax.experimental import pallas as pl
from jax.experimental.pallas import tpu as pltpu
from jax.sharding import PartitionSpec as P

AXES = ("row", "col")
DEVICES = 256
SEQS = 2
BLOCK = 128
D = 2048
LEAVE = 4
PARTS = D // LEAVE
GROUPS = 8
GROUP_DIM = 128
FW = GROUPS * GROUP_DIM
TWO = 2 * GROUP_DIM
LENGTH = 32768
PAIRS = 4
ROWS = 2 * PAIRS
NT = (((1,), (1,)), ((), ()))
TN = (((0,), (0,)), ((), ()))
F32, BF16 = jnp.float32, jnp.bfloat16
ENTER = 512
SMALL = pltpu.CompilerParams(vmem_limit_bytes=16 * 2**20)


def in_hbm(x):
    return pltpu.with_memory_space_constraint(x, pltpu.HBM)


def in_vmem(x):
    return pltpu.with_memory_space_constraint(x, pltpu.VMEM)


def group_table():
    table = np.zeros((GROUP_DIM, GROUP_DIM))
    j = np.arange(GROUP_DIM)
    for i in range(GROUP_DIM // ROWS):
        for p in range(PAIRS):
            k = PAIRS * i + p
            table[i * ROWS + p] = np.cos(2 * np.pi * j * k / GROUP_DIM)
            table[i * ROWS + PAIRS + p] = np.sin(2 * np.pi * j * k / GROUP_DIM)
    table[PAIRS] = np.cos(np.pi * j)
    return table / 8


def channel_order():
    order = np.zeros((GROUP_DIM, GROUP_DIM))
    for i in range(GROUP_DIM // ROWS):
        for p in range(PAIRS):
            k = PAIRS * i + p
            order[i * ROWS + p, k] = 1
            order[i * ROWS + PAIRS + p, (GROUP_DIM - k) if k else GROUP_DIM // 2] = 1
    return order


def first_table():
    m, d = np.arange(DEVICES)[:, None], np.arange(DEVICES)[None, :]
    angle = 2 * np.pi * (m * d % DEVICES) / DEVICES
    return np.concatenate([np.cos(angle), np.sin(angle)], axis=0) / 16


def twiddle():
    m, l = np.arange(DEVICES)[:, None], np.arange(BLOCK)[None, :]
    angle = 2 * np.pi * (m * l) / LENGTH
    return np.stack([np.cos(angle), np.sin(angle)])


def second_table():
    m, l = np.arange(BLOCK)[:, None], np.arange(BLOCK)[None, :]
    angle = 2 * np.pi * (m * l % BLOCK) / BLOCK
    return np.concatenate([np.cos(angle), -np.sin(angle)], axis=1) / 16


def enter_body(
    tokens, gain, weight, table, out, saved, held, scale, turn, normed, matrix, spectra, sems
):
    def load(source, target, at):
        copy = pltpu.make_async_copy(source, target, sems.at[at])
        copy.start()
        return copy

    small = [load(gain, scale, 0), load(table, turn, 1)]
    rows_in = [load(tokens.at[s], held.at[s], 2 + s) for s in range(SEQS)]
    cuts = [slice(c * ENTER, (c + 1) * ENTER) for c in range(FW // ENTER)]
    chunks = [load(weight.at[:, cut], matrix.at[:, cut], 4 + c) for c, cut in enumerate(cuts)]
    for copy in small:
        copy.wait()
    for s in range(SEQS):
        rows_in[s].wait()

        def rows(i, _):
            at = pl.ds(pl.multiple_of(i * 16, 16), 16)
            t = held[s, at, :].astype(F32)
            inv = lax.rsqrt(jnp.mean(t * t, axis=-1, keepdims=True) + 1e-6)
            to = pl.ds(pl.multiple_of(s * BLOCK + i * 16, 16), 16)
            normed[to, :] = (t * inv * scale[...]).astype(BF16)
            return 0

        lax.fori_loop(0, BLOCK // 16, rows, 0, unroll=8)
    saves = []
    for chunk, cut in zip(chunks, cuts):
        chunk.wait()
        if cut.stop == FW:
            saves.append(load(normed, saved, 4 + len(cuts) + len(saves)))
        mixed = jnp.dot(normed[...], matrix[:, cut], preferred_element_type=F32).astype(BF16)
        for q in range(ENTER // TWO):
            part = mixed[:, q * TWO : (q + 1) * TWO]
            turned = lax.dot_general(turn[...], part, NT, preferred_element_type=F32)
            at = slice(cut.start + q * TWO, cut.start + (q + 1) * TWO)
            for s in range(SEQS):
                spectra[s, at, :] = turned[:, s * BLOCK : (s + 1) * BLOCK].astype(BF16)
        saves.append(load(spectra.at[:, cut], out.at[:, cut], 4 + len(cuts) + len(saves)))
    for save in saves:
        save.wait()


def enter(tokens, gain, weight):
    hbm = pl.BlockSpec(memory_space=pltpu.HBM)
    return pl.pallas_call(
        enter_body,
        in_specs=[hbm] * 4,
        out_specs=[hbm, hbm],
        out_shape=[
            pltpu.HBM((SEQS, FW, BLOCK), BF16),
            pltpu.HBM((SEQS * BLOCK, D), BF16),
        ],
        scratch_shapes=[
            pltpu.VMEM((SEQS, BLOCK, D), BF16),
            pltpu.VMEM((1, D), F32),
            pltpu.VMEM((TWO, TWO), BF16),
            pltpu.VMEM((SEQS * BLOCK, D), BF16),
            pltpu.VMEM((D, FW), BF16),
            pltpu.VMEM((SEQS, FW, BLOCK), BF16),
            pltpu.SemaphoreType.DMA((5 + 2 * (FW // ENTER),)),
        ],
        compiler_params=SMALL,
        name="enter",
    )(
        in_hbm(tokens),
        in_hbm(gain.reshape(1, D)),
        in_hbm(weight),
        in_hbm(jnp.asarray(np.kron(np.eye(2), group_table()), BF16)),
    )


def length_body(lone, x, first, twist, second, later, y, kept, wide_in, wide_out, sem):
    load = pltpu.make_async_copy(later.at[:, PARTS : 2 * PARTS], kept, sem)
    load.start()

    @pl.when(lone[0] >= 0)
    def _():
        over_positions(lone[0], x, first, twist, second, y, wide_in, wide_out)

    load.wait()


def over_positions(own, x, first, twist, second, y, wide_in, wide_out):
    wide_in[...] = x[...].astype(F32)
    cos, sin = twist[0], twist[1]
    for p in range(PAIRS):
        pair = jnp.concatenate(
            [
                wide_in[pl.ds(p, DEVICES, stride=ROWS), :].astype(BF16),
                wide_in[pl.ds(PAIRS + p, DEVICES, stride=ROWS), :].astype(BF16),
            ],
            axis=1,
        )
        both = jnp.dot(first[...], pair, preferred_element_type=F32)
        parts = []
        for q in range(2):
            real = both[:DEVICES, q * BLOCK : (q + 1) * BLOCK]
            imag = both[DEVICES:, q * BLOCK : (q + 1) * BLOCK]
            if q == 0:
                c, s = cos, sin
            elif p == 0:
                c, s = own * cos + (1 - own) * sin, own * sin - (1 - own) * cos
            else:
                c, s = sin, -cos
            turned = jnp.concatenate(
                [(real * c - imag * s).astype(BF16), (real * s + imag * c).astype(BF16)], axis=1
            )
            parts.append(lax.dot_general(second[...], turned, NT, preferred_element_type=F32))
        if p == 0:
            low, high = parts[0] - (1 - own) * parts[1], (1 - own) * parts[0] + parts[1]
        else:
            low, high = parts[0] - parts[1], parts[0] + parts[1]
        for h in range(2):
            at = slice(h * BLOCK, (h + 1) * BLOCK)
            wide_out[pl.ds(h * ROWS + p, BLOCK, stride=2 * ROWS), :] = low[:, at]
            wide_out[pl.ds(h * ROWS + PAIRS + p, BLOCK, stride=2 * ROWS), :] = high[:, at]
    y[...] = wide_out[...].astype(BF16)


def length_transform(x, lone, later):
    vmem = pl.BlockSpec(memory_space=pltpu.VMEM)
    rows = DEVICES * ROWS
    return pl.pallas_call(
        length_body,
        in_specs=[
            pl.BlockSpec(memory_space=pltpu.SMEM),
            vmem,
            vmem,
            vmem,
            vmem,
            pl.BlockSpec(memory_space=pltpu.HBM),
        ],
        out_specs=[vmem, vmem],
        out_shape=[jax.ShapeDtypeStruct((rows, BLOCK), BF16), pltpu.VMEM((FW, PARTS), BF16)],
        scratch_shapes=[
            pltpu.VMEM((rows, BLOCK), F32),
            pltpu.VMEM((rows, BLOCK), F32),
            pltpu.SemaphoreType.DMA,
        ],
        compiler_params=SMALL,
        name="length",
    )(
        lone,
        x,
        jnp.asarray(first_table(), BF16),
        jnp.asarray(twiddle(), F32),
        jnp.asarray(second_table(), BF16),
        in_hbm(later),
    )


LATE = [slice(c * PARTS, (c + 1) * PARTS) for c in range(2, LEAVE)]


def gate_body(normed, weight, later, out, kept, *refs):
    loads = [pltpu.make_async_copy(later.at[:, :PARTS], kept, refs[-1].at[0])]
    for c, cut in enumerate(LATE):
        loads.append(pltpu.make_async_copy(later.at[:, cut], refs[c], refs[-1].at[1 + c]))

    @pl.when(pl.program_id(0) == 0)
    def _():
        for load in loads:
            load.start()

    logits = jnp.dot(normed[...], weight[...], preferred_element_type=F32)
    out[...] = jax.nn.sigmoid(logits).astype(BF16)

    @pl.when(pl.program_id(0) == pl.num_programs(0) - 1)
    def _():
        for load in loads:
            load.wait()


def gate(normed, weight, later):
    steps = 8
    wide = D // steps
    hbm = pl.BlockSpec(memory_space=pltpu.HBM)
    return pl.pallas_call(
        gate_body,
        grid=(steps,),
        in_specs=[
            pl.BlockSpec((SEQS * BLOCK, D), lambda j: (0, 0)),
            pl.BlockSpec((D, wide), lambda j: (0, j)),
            hbm,
        ],
        out_specs=[
            pl.BlockSpec((SEQS * BLOCK, wide), lambda j: (0, j)),
            pl.BlockSpec(memory_space=pltpu.VMEM),
        ]
        + [hbm] * len(LATE),
        out_shape=[pltpu.VMEM((SEQS * BLOCK, D), BF16), pltpu.VMEM((FW, PARTS), BF16)]
        + [pltpu.HBM((FW, PARTS), BF16)] * len(LATE),
        scratch_shapes=[pltpu.SemaphoreType.DMA((1 + len(LATE),))],
        cost_estimate=pl.CostEstimate(
            flops=2 * SEQS * BLOCK * D * D, transcendentals=SEQS * BLOCK * D, bytes_accessed=2 * D * D
        ),
        compiler_params=SMALL,
        name="gate",
    )(in_hbm(normed), in_hbm(weight), in_hbm(later))


def leave_body(z, order, gates, *refs):
    parts, (out, spectral, gated, sems) = refs[:LEAVE], refs[LEAVE:]
    for g in range(FW // TWO):
        for s in range(SEQS):
            rows = z[s * FW + g * TWO : s * FW + (g + 1) * TWO, :]
            placed = lax.dot_general(rows, order[...], TN, preferred_element_type=F32)
            spectral[s * BLOCK : (s + 1) * BLOCK, g * TWO : (g + 1) * TWO] = placed.astype(BF16)
    copies = []
    for c in range(LEAVE):
        at = slice(c * PARTS, (c + 1) * PARTS)
        mapped = jnp.dot(spectral[...], parts[c][...], preferred_element_type=F32)
        block = (gates[:, at].astype(F32) * mapped).astype(BF16)
        for s in range(SEQS):
            gated[s, :, at] = block[s * BLOCK : (s + 1) * BLOCK]
        copy = pltpu.make_async_copy(gated.at[:, :, at], out.at[:, :, at], sems.at[c])
        copy.start()
        copies.append(copy)
    for copy in copies:
        copy.wait()


def leave(z, gates, *parts):
    vmem = pl.BlockSpec(memory_space=pltpu.VMEM)
    return pl.pallas_call(
        leave_body,
        in_specs=[vmem] * (3 + len(parts)),
        out_specs=pl.BlockSpec(memory_space=pltpu.HBM),
        out_shape=jax.ShapeDtypeStruct((SEQS, BLOCK, D), BF16),
        scratch_shapes=[
            pltpu.VMEM((SEQS * BLOCK, FW), BF16),
            pltpu.VMEM((SEQS, BLOCK, D), BF16),
            pltpu.SemaphoreType.DMA((LEAVE,)),
        ],
        compiler_params=SMALL,
        name="leave",
    )(
        z,
        jnp.asarray(np.kron(np.eye(2), channel_order()), BF16),
        *(in_vmem(held) for held in (gates, *parts)),
    )


def exchange(x):
    return lax.all_to_all(x.reshape(DEVICES, ROWS, BLOCK), AXES, 0, 0, tiled=True).reshape(
        DEVICES * ROWS, BLOCK
    )


def local(tokens, norm_gain, mix_weight, gate_weight, out_weight):
    spectra, normed = enter(tokens, norm_gain, mix_weight)
    lone = (lax.axis_index(AXES) % (GROUP_DIM // ROWS) == 0).astype(F32).reshape(1)
    arrived = exchange(spectra)
    arrived, (gates, part_0, *late) = lax.optimization_barrier(
        (arrived, gate(normed, gate_weight, out_weight))
    )
    turned, part_1 = length_transform(arrived, lone, out_weight)
    return leave(exchange(turned), gates, part_0, part_1, *late)


def solution(mesh):
    return jax.shard_map(
        local,
        mesh=mesh,
        in_specs=(P(None, AXES, None), P(), P(), P(), P()),
        out_specs=P(None, AXES, None),
        check_vma=False,
    )
```

```python
import jax
import jax.numpy as jnp
import numpy as np
from jax import lax
from jax.experimental import pallas as pl
from jax.experimental.pallas import tpu as pltpu
from jax.sharding import PartitionSpec as P

AXES = ("row", "col")
DEVICES = 256
SEQS = 2
BLOCK = 128
D = 2048
LEAVE = 4
PARTS = D // LEAVE
GROUPS = 8
GROUP_DIM = 128
FW = GROUPS * GROUP_DIM
TWO = 2 * GROUP_DIM
LENGTH = 32768
PAIRS = 4
ROWS = 2 * PAIRS
NT = (((1,), (1,)), ((), ()))
TN = (((0,), (0,)), ((), ()))
F32, BF16 = jnp.float32, jnp.bfloat16
ENTER = 512
SMALL = pltpu.CompilerParams(vmem_limit_bytes=16 * 2**20)


def in_hbm(x):
    return pltpu.with_memory_space_constraint(x, pltpu.HBM)


def in_vmem(x):
    return pltpu.with_memory_space_constraint(x, pltpu.VMEM)


def group_table():
    table = np.zeros((GROUP_DIM, GROUP_DIM))
    j = np.arange(GROUP_DIM)
    for i in range(GROUP_DIM // ROWS):
        for p in range(PAIRS):
            k = PAIRS * i + p
            table[i * ROWS + p] = np.cos(2 * np.pi * j * k / GROUP_DIM)
            table[i * ROWS + PAIRS + p] = np.sin(2 * np.pi * j * k / GROUP_DIM)
    table[PAIRS] = np.cos(np.pi * j)
    return table / 8


def channel_order():
    order = np.zeros((GROUP_DIM, GROUP_DIM))
    for i in range(GROUP_DIM // ROWS):
        for p in range(PAIRS):
            k = PAIRS * i + p
            order[i * ROWS + p, k] = 1
            order[i * ROWS + PAIRS + p, (GROUP_DIM - k) if k else GROUP_DIM // 2] = 1
    return order


def first_table():
    m, d = np.arange(DEVICES)[:, None], np.arange(DEVICES)[None, :]
    angle = 2 * np.pi * (m * d % DEVICES) / DEVICES
    return np.concatenate([np.cos(angle), np.sin(angle)], axis=0) / 16


def twiddle():
    m, l = np.arange(DEVICES)[:, None], np.arange(BLOCK)[None, :]
    angle = 2 * np.pi * (m * l) / LENGTH
    return np.stack([np.cos(angle), np.sin(angle)])


def second_table():
    m, l = np.arange(BLOCK)[:, None], np.arange(BLOCK)[None, :]
    angle = 2 * np.pi * (m * l % BLOCK) / BLOCK
    return np.concatenate([np.cos(angle), -np.sin(angle)], axis=1) / 16


def enter_body(
    tokens, gain, weight, table, out, saved, held, scale, turn, normed, matrix, spectra, sems
):
    def load(source, target, at):
        copy = pltpu.make_async_copy(source, target, sems.at[at])
        copy.start()
        return copy

    small = [load(gain, scale, 0), load(table, turn, 1)]
    rows_in = [load(tokens.at[s], held.at[s], 2 + s) for s in range(SEQS)]
    cuts = [slice(c * ENTER, (c + 1) * ENTER) for c in range(FW // ENTER)]
    chunks = [load(weight.at[:, cut], matrix.at[:, cut], 4 + c) for c, cut in enumerate(cuts)]
    for copy in small:
        copy.wait()
    for s in range(SEQS):
        rows_in[s].wait()

        def rows(i, _):
            at = pl.ds(pl.multiple_of(i * 16, 16), 16)
            t = held[s, at, :].astype(F32)
            inv = lax.rsqrt(jnp.mean(t * t, axis=-1, keepdims=True) + 1e-6)
            to = pl.ds(pl.multiple_of(s * BLOCK + i * 16, 16), 16)
            normed[to, :] = (t * inv * scale[...]).astype(BF16)
            return 0

        lax.fori_loop(0, BLOCK // 16, rows, 0, unroll=8)
    saves = []
    for chunk, cut in zip(chunks, cuts):
        chunk.wait()
        if cut.stop == FW:
            saves.append(load(normed, saved, 4 + len(cuts) + len(saves)))
        mixed = jnp.dot(normed[...], matrix[:, cut], preferred_element_type=F32).astype(BF16)
        for q in range(ENTER // TWO):
            part = mixed[:, q * TWO : (q + 1) * TWO]
            turned = lax.dot_general(turn[...], part, NT, preferred_element_type=F32)
            at = slice(cut.start + q * TWO, cut.start + (q + 1) * TWO)
            for s in range(SEQS):
                spectra[s, at, :] = turned[:, s * BLOCK : (s + 1) * BLOCK].astype(BF16)
        saves.append(load(spectra.at[:, cut], out.at[:, cut], 4 + len(cuts) + len(saves)))
    for save in saves:
        save.wait()


def enter(tokens, gain, weight):
    hbm = pl.BlockSpec(memory_space=pltpu.HBM)
    return pl.pallas_call(
        enter_body,
        in_specs=[hbm] * 4,
        out_specs=[hbm, hbm],
        out_shape=[
            pltpu.HBM((SEQS, FW, BLOCK), BF16),
            pltpu.HBM((SEQS * BLOCK, D), BF16),
        ],
        scratch_shapes=[
            pltpu.VMEM((SEQS, BLOCK, D), BF16),
            pltpu.VMEM((1, D), F32),
            pltpu.VMEM((TWO, TWO), BF16),
            pltpu.VMEM((SEQS * BLOCK, D), BF16),
            pltpu.VMEM((D, FW), BF16),
            pltpu.VMEM((SEQS, FW, BLOCK), BF16),
            pltpu.SemaphoreType.DMA((5 + 2 * (FW // ENTER),)),
        ],
        compiler_params=SMALL,
        name="enter",
    )(
        in_hbm(tokens),
        in_hbm(gain.reshape(1, D)),
        in_hbm(weight),
        in_hbm(jnp.asarray(np.kron(np.eye(2), group_table()), BF16)),
    )


def length_body(lone, x, first, twist, second, later, y, kept, wide_in, wide_out, sem):
    load = pltpu.make_async_copy(later.at[:, PARTS : 2 * PARTS], kept, sem)
    load.start()

    @pl.when(lone[0] >= 0)
    def _():
        over_positions(lone[0], x, first, twist, second, y, wide_in, wide_out)

    load.wait()


def over_positions(own, x, first, twist, second, y, wide_in, wide_out):
    wide_in[...] = x[...].astype(F32)
    cos, sin = twist[0], twist[1]
    for p in range(PAIRS):
        pair = jnp.concatenate(
            [
                wide_in[pl.ds(p, DEVICES, stride=ROWS), :].astype(BF16),
                wide_in[pl.ds(PAIRS + p, DEVICES, stride=ROWS), :].astype(BF16),
            ],
            axis=1,
        )
        both = jnp.dot(first[...], pair, preferred_element_type=F32)
        parts = []
        for q in range(2):
            real = both[:DEVICES, q * BLOCK : (q + 1) * BLOCK]
            imag = both[DEVICES:, q * BLOCK : (q + 1) * BLOCK]
            if q == 0:
                c, s = cos, sin
            elif p == 0:
                c, s = own * cos + (1 - own) * sin, own * sin - (1 - own) * cos
            else:
                c, s = sin, -cos
            turned = jnp.concatenate(
                [(real * c - imag * s).astype(BF16), (real * s + imag * c).astype(BF16)], axis=1
            )
            parts.append(lax.dot_general(second[...], turned, NT, preferred_element_type=F32))
        if p == 0:
            low, high = parts[0] - (1 - own) * parts[1], (1 - own) * parts[0] + parts[1]
        else:
            low, high = parts[0] - parts[1], parts[0] + parts[1]
        for h in range(2):
            at = slice(h * BLOCK, (h + 1) * BLOCK)
            wide_out[pl.ds(h * ROWS + p, BLOCK, stride=2 * ROWS), :] = low[:, at]
            wide_out[pl.ds(h * ROWS + PAIRS + p, BLOCK, stride=2 * ROWS), :] = high[:, at]
    y[...] = wide_out[...].astype(BF16)


def length_transform(x, lone, later):
    vmem = pl.BlockSpec(memory_space=pltpu.VMEM)
    rows = DEVICES * ROWS
    return pl.pallas_call(
        length_body,
        in_specs=[
            pl.BlockSpec(memory_space=pltpu.SMEM),
            vmem,
            vmem,
            vmem,
            vmem,
            pl.BlockSpec(memory_space=pltpu.HBM),
        ],
        out_specs=[vmem, vmem],
        out_shape=[jax.ShapeDtypeStruct((rows, BLOCK), BF16), pltpu.VMEM((FW, PARTS), BF16)],
        scratch_shapes=[
            pltpu.VMEM((rows, BLOCK), F32),
            pltpu.VMEM((rows, BLOCK), F32),
            pltpu.SemaphoreType.DMA,
        ],
        compiler_params=SMALL,
        name="length",
    )(
        lone,
        x,
        jnp.asarray(first_table(), BF16),
        jnp.asarray(twiddle(), F32),
        jnp.asarray(second_table(), BF16),
        in_hbm(later),
    )


LATE = [slice(c * PARTS, (c + 1) * PARTS) for c in range(2, LEAVE)]


def gate_body(normed, weight, later, out, kept, *refs):
    cut_off, (passing, sems) = refs[:-2], refs[-2:]
    own = pltpu.make_async_copy(later.at[:, :PARTS], kept, sems.at[0])
    loads, stores = [], []
    for c, cut in enumerate(LATE):
        loads.append(pltpu.make_async_copy(later.at[:, cut], passing.at[c], sems.at[1 + c]))
        stores.append(pltpu.make_async_copy(passing.at[c], cut_off[c], sems.at[LEAVE + c]))

    @pl.when(pl.program_id(0) == 0)
    def _():
        for load in (*loads, own):
            load.start()

    logits = jnp.dot(normed[...], weight[...], preferred_element_type=F32)
    out[...] = jax.nn.sigmoid(logits).astype(BF16)

    @pl.when(pl.program_id(0) == pl.num_programs(0) // 2)
    def _():
        for load, store in zip(loads, stores):
            load.wait()
            store.start()

    @pl.when(pl.program_id(0) == pl.num_programs(0) - 1)
    def _():
        for copy in (own, *stores):
            copy.wait()


def gate(normed, weight, later):
    steps = 8
    wide = D // steps
    hbm = pl.BlockSpec(memory_space=pltpu.HBM)
    return pl.pallas_call(
        gate_body,
        grid=(steps,),
        in_specs=[
            pl.BlockSpec((SEQS * BLOCK, D), lambda j: (0, 0)),
            pl.BlockSpec((D, wide), lambda j: (0, j)),
            hbm,
        ],
        out_specs=[
            pl.BlockSpec((SEQS * BLOCK, wide), lambda j: (0, j)),
            pl.BlockSpec(memory_space=pltpu.VMEM),
        ]
        + [hbm] * len(LATE),
        out_shape=[pltpu.VMEM((SEQS * BLOCK, D), BF16), pltpu.VMEM((FW, PARTS), BF16)]
        + [pltpu.HBM((FW, PARTS), BF16)] * len(LATE),
        scratch_shapes=[
            pltpu.VMEM((len(LATE), FW, PARTS), BF16),
            pltpu.SemaphoreType.DMA((2 * LEAVE,)),
        ],
        cost_estimate=pl.CostEstimate(
            flops=2 * SEQS * BLOCK * D * D, transcendentals=SEQS * BLOCK * D, bytes_accessed=2 * D * D
        ),
        compiler_params=SMALL,
        name="gate",
    )(in_hbm(normed), in_hbm(weight), in_hbm(later))


def leave_body(z, order, gates, *refs):
    parts, (out, spectral, gated, sems) = refs[:LEAVE], refs[LEAVE:]
    for g in range(FW // TWO):
        for s in range(SEQS):
            rows = z[s * FW + g * TWO : s * FW + (g + 1) * TWO, :]
            placed = lax.dot_general(rows, order[...], TN, preferred_element_type=F32)
            spectral[s * BLOCK : (s + 1) * BLOCK, g * TWO : (g + 1) * TWO] = placed.astype(BF16)
    copies = []
    for c in range(LEAVE):
        at = slice(c * PARTS, (c + 1) * PARTS)
        mapped = jnp.dot(spectral[...], parts[c][...], preferred_element_type=F32)
        block = (gates[:, at].astype(F32) * mapped).astype(BF16)
        for s in range(SEQS):
            gated[s, :, at] = block[s * BLOCK : (s + 1) * BLOCK]
        copy = pltpu.make_async_copy(gated.at[:, :, at], out.at[:, :, at], sems.at[c])
        copy.start()
        copies.append(copy)
    for copy in copies:
        copy.wait()


def leave(z, gates, *parts):
    vmem = pl.BlockSpec(memory_space=pltpu.VMEM)
    return pl.pallas_call(
        leave_body,
        in_specs=[vmem] * (3 + len(parts)),
        out_specs=pl.BlockSpec(memory_space=pltpu.HBM),
        out_shape=jax.ShapeDtypeStruct((SEQS, BLOCK, D), BF16),
        scratch_shapes=[
            pltpu.VMEM((SEQS * BLOCK, FW), BF16),
            pltpu.VMEM((SEQS, BLOCK, D), BF16),
            pltpu.SemaphoreType.DMA((LEAVE,)),
        ],
        compiler_params=SMALL,
        name="leave",
    )(
        z,
        jnp.asarray(np.kron(np.eye(2), channel_order()), BF16),
        *(in_vmem(held) for held in (gates, *parts)),
    )


def exchange(x):
    return lax.all_to_all(x.reshape(DEVICES, ROWS, BLOCK), AXES, 0, 0, tiled=True).reshape(
        DEVICES * ROWS, BLOCK
    )


def local(tokens, norm_gain, mix_weight, gate_weight, out_weight):
    spectra, normed = enter(tokens, norm_gain, mix_weight)
    lone = (lax.axis_index(AXES) % (GROUP_DIM // ROWS) == 0).astype(F32).reshape(1)
    arrived = exchange(spectra)
    arrived, (gates, part_0, *late) = lax.optimization_barrier(
        (arrived, gate(normed, gate_weight, out_weight))
    )
    turned, part_1 = length_transform(arrived, lone, out_weight)
    return leave(exchange(turned), gates, part_0, part_1, *late)


def solution(mesh):
    return jax.shard_map(
        local,
        mesh=mesh,
        in_specs=(P(None, AXES, None), P(), P(), P(), P()),
        out_specs=P(None, AXES, None),
        check_vma=False,
    )
```
